256 devices in a mesh: grp: 2 (over y), sp: 32 (over z, core), tp: 4 (over x).
Axes of the slice: x: 4, y: 2, z: 16, core: 2. Of those that a mesh axis runs over, the one named last changes fastest.
The devices are a block of a 4x16x16 slice.
Arguments:
- residual: bfloat16 [45056, 2048], P(('grp', 'sp')), parts along dimension 0, may hold values from -6 to 6
- mix_input: bfloat16 [45056, 2048], P(('grp', 'sp'), 'tp'), parts along dimension 0, may hold values from -6 to 6
- gate_input: bfloat16 [45056, 2048], P(('grp', 'sp'), 'tp'), parts along dimension 0, may hold values from -6 to 6
- mix_kernel: bfloat16 [4, 2048], P(None, 'tp'), may hold values from -3 to 3
- recur_gate_map: bfloat16 [16, 128, 128], P('tp'), may hold values from -0.5 to 0.5
- input_gate_map: bfloat16 [16, 128, 128], P('tp'), may hold values from -0.5 to 0.5
- decay_param: float32 [2048], P('tp')
- jump_log: float32 [45056, 2048], P(('grp', 'sp'), 'tp'), parts along dimension 0, may hold values from -2.1 to 0
- out_weight: bfloat16 [2048, 2048], P('tp'), may hold values from -0.125 to 0.125
- mix_gain: float32 [2048], replicated, may hold values from 0.1 to 1.9
- inner_gain: float32 [2048], replicated, may hold values from 0.1 to 1.9
- final_gain: float32 [2048], replicated, may hold values from 0.1 to 1.9
- gate_weight: bfloat16 [2048, 5632], P('sp', 'tp'), may hold values from -0.125 to 0.125
- value_weight: bfloat16 [2048, 5632], P('sp', 'tp'), may hold values from -0.125 to 0.125
- gate_kernel: bfloat16 [3, 5632], P(None, 'tp'), may hold values from -3.5 to 3.5
- value_kernel: bfloat16 [3, 5632], P(None, 'tp'), may hold values from -3.5 to 3.5
- down_weight: bfloat16 [5632, 2048], P('tp', 'sp'), may hold values from -0.078125 to 0.078125
Outputs:
- layer_output: bfloat16 [45056, 2048], P(('grp', 'sp', 'tp')), parts along dimension 0
The draws below stay inside these ranges and needn't reach their ends.
There are 2 independent parts, one for each index of `grp`. The reference program is written for one: setup_inputs(seed, part) draws one part's arguments, and reference() takes and returns one part's arrays. A program takes and returns all parts, laid end to end along the dimension named above; an argument that names none is the same for every part. Nothing has to cross between parts.
All inputs are finite; a program needn't handle non-finite values.
Results may differ from the reference program's by a relative error of at most 0.02.
Values may be sent and summed in bfloat16 or wider, within the bound.
A program may use at most 128 MiB of HBM per device.

```python
import jax
import jax.numpy as jnp
from jax import lax

D = 2048
BW = 128
NB = 16
FF = 5632
MIX_TAPS = 4
HIDDEN_TAPS = 3
TOK_DEV = 704
TOKENS = 22528
N_TP = 4


def draw_decay_param(key, part):
    fast_share = 0.5
    fast = jax.random.uniform(jax.random.fold_in(key, 11), (D,), jnp.float32) < fast_share
    fast_rate = jnp.exp(jax.random.uniform(jax.random.fold_in(key, 12), (D,), jnp.float32, jnp.log(0.008), jnp.log(0.03)))
    slow_rate = jnp.exp(jax.random.uniform(jax.random.fold_in(key, 13), (D,), jnp.float32, jnp.log(0.03), jnp.log(0.12))) / TOKENS
    rate = jnp.where(fast, fast_rate, slow_rate)
    return (-jnp.log(jnp.expm1(rate))).astype(jnp.float32)


def draw_jump_log(key, part):
    block_count = TOKENS // TOK_DEV
    factor = jnp.exp(jax.random.uniform(jax.random.fold_in(key, 21), (block_count, D), jnp.float32, jnp.log(0.3), jnp.log(3.0)))
    steady = jnp.repeat(-0.3 * factor / TOKENS, TOK_DEV, axis=0)
    spots = jax.random.randint(jax.random.fold_in(key, 22), (3,), 0, TOKENS)
    depth = jnp.log(jax.random.uniform(jax.random.fold_in(key, 23), (3, D), jnp.float32, 0.5, 0.8))
    hits = (jnp.arange(TOKENS)[:, None] == spots[None, :]).astype(jnp.float32)
    return (steady + jnp.dot(hits, depth)).astype(jnp.float32)


def block_levels(own_key, extent, pieces, low, high):
    loudness, own = 1.0, jax.random.fold_in(own_key, 6)
    for axis_at, shards_of in pieces:
        heights = jnp.exp(jax.random.uniform(jax.random.fold_in(own, axis_at), (shards_of,), jnp.float32, low / len(pieces), high / len(pieces)))
        loudness = loudness * jnp.repeat(heights, extent[axis_at] // shards_of).reshape([-1 if axis == axis_at else 1 for axis in range(len(extent))])
    return loudness


def normal_values(rng, shape, scale, limit, pieces=(), dtype=jnp.bfloat16):
    entries = scale * jax.random.normal(rng, shape, jnp.float32)
    if pieces:
        entries = entries * block_levels(rng, shape, pieces, -0.22, 0.18)
    return jnp.clip(entries, -limit, limit).astype(dtype)


def setup_inputs(seed: int = 0, part: int = 0) -> dict:
    key_of = jax.random.split(jax.random.key(seed), 18)
    part_keys = jax.random.split(jax.random.fold_in(key_of[17], part), 18)
    return {
        "residual": normal_values(part_keys[0], (TOKENS, D), 1.0, 6.0, ((0, 32),)),
        "mix_input": normal_values(part_keys[1], (TOKENS, D), 1.0, 6.0, ((0, 32), (1, 4))),
        "gate_input": normal_values(part_keys[2], (TOKENS, D), 1.0, 6.0, ((0, 32), (1, 4))),
        "mix_kernel": normal_values(key_of[3], (MIX_TAPS, D), MIX_TAPS ** -0.5, 3.0, ((1, 4),)),
        "recur_gate_map": normal_values(key_of[4], (NB, BW, BW), BW ** -0.5, 0.5, ((0, 4),)),
        "input_gate_map": normal_values(key_of[5], (NB, BW, BW), BW ** -0.5, 0.5, ((0, 4),)),
        "decay_param": draw_decay_param(jax.random.fold_in(key_of[17], 71), part),
        "jump_log": draw_jump_log(jax.random.fold_in(jax.random.fold_in(key_of[17], part), 71), part),
        "out_weight": normal_values(key_of[8], (D, D), D ** -0.5, 0.125, ((0, 4),)),
        "mix_gain": jnp.clip(1.0 + 0.18 * jax.random.normal(key_of[9], (D,), jnp.float32), 0.1, 1.9),
        "inner_gain": jnp.clip(1.0 + 0.18 * jax.random.normal(key_of[10], (D,), jnp.float32), 0.1, 1.9),
        "final_gain": jnp.clip(1.0 + 0.18 * jax.random.normal(key_of[11], (D,), jnp.float32), 0.1, 1.9),
        "gate_weight": normal_values(key_of[12], (D, FF), D ** -0.5, 0.125, ((0, 32), (1, 4))),
        "value_weight": normal_values(key_of[13], (D, FF), D ** -0.5, 0.125, ((0, 32), (1, 4))),
        "gate_kernel": normal_values(key_of[14], (HIDDEN_TAPS, FF), HIDDEN_TAPS ** -0.5, 3.5, ((1, 4),)),
        "value_kernel": normal_values(key_of[15], (HIDDEN_TAPS, FF), HIDDEN_TAPS ** -0.5, 3.5, ((1, 4),)),
        "down_weight": normal_values(key_of[16], (FF, D), FF ** -0.5, 0.078125, ((0, 4), (1, 32))),
    }


EPS = 1e-06
GATE_SCALE = 8.0

def norm_scale(values, gain_vec):
    values = values.astype(jnp.float32)
    return values * lax.rsqrt(lax.optimization_barrier(jnp.mean(values * values, axis=-1, keepdims=True)) + EPS) * gain_vec

def causal_taps(padded, kernel, length):
    kernel = kernel.astype(jnp.float32)
    result = jnp.zeros((length, padded.shape[1]), jnp.float32)
    for offset in range(kernel.shape[0]):
        result = result + padded[offset:offset + length] * kernel[offset]
    return result

def linear_pair(before_pair, after_pair):
    return (before_pair[0] * after_pair[0], after_pair[0] * before_pair[1] + after_pair[1])

def rounded(values):
    return lax.optimization_barrier(values.astype(jnp.bfloat16)).astype(jnp.float32)

def group_sum(activations, weights, groups):
    group_width = activations.shape[1] // groups
    running = jnp.zeros((activations.shape[0], weights.shape[1]), jnp.float32)
    for group_index in range(groups):
        lower = group_index * group_width
        running = running + rounded(jnp.dot(activations[:, lower:lower + group_width], weights[lower:lower + group_width], preferred_element_type=jnp.float32))
    return running

def reference(residual, mix_input, gate_input, mix_kernel, recur_gate_map, input_gate_map, decay_param, jump_log, out_weight, mix_gain, inner_gain, final_gain, gate_weight, value_weight, gate_kernel, value_kernel, down_weight):
    length = mix_input.shape[0]
    padded = jnp.pad(mix_input.astype(jnp.float32), ((MIX_TAPS - 1, 0), (0, 0)))
    conv_rows = causal_taps(padded, mix_kernel, length).astype(jnp.bfloat16)
    grouped = conv_rows.astype(jnp.float32).reshape(length, NB, BW)
    recur_gate = jax.nn.sigmoid(jnp.einsum('tnd,nde->tne', grouped, recur_gate_map.astype(jnp.float32))).reshape(length, D)
    input_gate = jax.nn.sigmoid(jnp.einsum('tnd,nde->tne', grouped, input_gate_map.astype(jnp.float32))).reshape(length, D)
    log_decay = -GATE_SCALE * recur_gate * jax.nn.softplus(-decay_param) + jump_log
    drive = jnp.sqrt(-jnp.expm1(2.0 * log_decay)) * input_gate * conv_rows.astype(jnp.float32)
    ignored, state = lax.associative_scan(linear_pair, (jnp.exp(log_decay), drive), axis=0)
    branch = (state * jax.nn.gelu(gate_input.astype(jnp.float32), approximate=True)).astype(jnp.bfloat16)
    mixed = group_sum(branch, out_weight, N_TP).astype(jnp.bfloat16)
    hidden_state = (residual.astype(jnp.float32) + norm_scale(mixed, mix_gain)).astype(jnp.bfloat16)
    normed = norm_scale(hidden_state, inner_gain).astype(jnp.bfloat16)
    up_gate = jnp.dot(normed, gate_weight, preferred_element_type=jnp.float32).astype(jnp.bfloat16)
    up_value = jnp.dot(normed, value_weight, preferred_element_type=jnp.float32).astype(jnp.bfloat16)
    gate_conv = causal_taps(jnp.pad(up_gate.astype(jnp.float32), ((HIDDEN_TAPS - 1, 0), (0, 0))), gate_kernel, length)
    value_conv = causal_taps(jnp.pad(up_value.astype(jnp.float32), ((HIDDEN_TAPS - 1, 0), (0, 0))), value_kernel, length)
    activation = (jax.nn.gelu(gate_conv, approximate=True) * value_conv).astype(jnp.bfloat16)
    down = group_sum(activation, down_weight, N_TP).astype(jnp.bfloat16)
    return (hidden_state.astype(jnp.float32) + norm_scale(down, final_gain)).astype(jnp.bfloat16)
```

```python
import functools

import jax
import jax.numpy as jnp
from jax import lax
from jax.experimental import pallas as pl
from jax.experimental.pallas import tpu as pltpu
from jax.sharding import PartitionSpec as P

EPS = 1e-06
GATE_SCALE = 8.0
LANES = 128
SEGMENTS = 8
TEAM = 8
SQRT_2_PI = 0.7978845608028654


def gelu(v):
    return 0.5 * v * (1.0 + jnp.tanh(SQRT_2_PI * (v + 0.044715 * (v * v * v))))


def sigmoid(v):
    return 1.0 / (1.0 + jnp.exp(-v))


def aligned(start, size, multiple):
    return pl.ds(pl.multiple_of(start, multiple), size)


def layer_kernel(
    num_sp,
    num_tp,
    mix_hbm,
    gate_hbm,
    jump_hbm,
    resid_hbm,
    outw_hbm,
    gw_hbm,
    vw_hbm,
    dw_hbm,
    mix_kernel,
    recur_map,
    input_map,
    coef,
    mix_gain,
    inner_gain,
    final_gain,
    gate_kernel,
    value_kernel,
    out_ref,
    wgv,
    wd,
    mixb,
    halo,
    gateb,
    a_s,
    b_s,
    gel,
    xpad,
    maps,
    branch,
    outw,
    resid,
    own_ab,
    team_ab,
    team_total,
    far_ab,
    rs1_send,
    rs1_recv,
    rs2_send,
    rs2_recv,
    mixed,
    hidden,
    normed,
    up,
    act,
    load_sem,
    wload_sem,
    halo_sem,
    tail_sem,
    team_send,
    team_recv,
    far_send,
    far_recv,
    ring_send,
    ring_recv,
    twin_send,
    twin_recv,
    rs1_ssem,
    rs1_rsem,
    rs2_ssem,
    rs2_rsem,
    ag_ssem,
    ag_rsem,
):
    sp = lax.axis_index("sp")
    t = lax.axis_index("tp")
    length, channels = mixb.shape
    groups = channels // LANES
    shard = gw_hbm.shape[0]
    width = gw_hbm.shape[1]
    tiles = width // LANES
    model = outw.shape[1]
    rows = length // num_tp
    half = model // 2
    sub = half // 2
    chips = num_sp // 2
    far = chips // 2
    core = lax.rem(sp, 2)
    chip = sp // 2
    twin = sp + 1 - 2 * core
    after = lax.rem(sp + 1, num_sp)
    before = lax.rem(sp + num_sp - 1, num_sp)
    z_next = (lax.rem(sp + 2, num_sp), lax.rem(sp + num_sp - 2, num_sp))
    t_next = (lax.rem(t + 1, num_tp), lax.rem(t + num_tp - 1, num_tp))
    place = lax.rem(sp, TEAM)
    team = sp // TEAM
    teams = num_sp // TEAM

    def sp_id(index):
        return {"sp": index}

    def tp_id(index):
        return {"tp": index}

    def mate(k):
        return team * TEAM + lax.rem(place + k, TEAM)

    def far_mate(k):
        return lax.rem(sp + TEAM * k, num_sp)

    barrier = pltpu.get_barrier_semaphore()
    partners = [sp_id(after), sp_id(before), sp_id(z_next[0]), sp_id(z_next[1])]
    partners += [sp_id(mate(k)) for k in range(1, TEAM)]
    partners += [sp_id(far_mate(k)) for k in range(1, teams)]
    partners += [tp_id(lax.rem(t + k, num_tp)) for k in range(1, num_tp)]
    for partner in partners:
        pl.semaphore_signal(barrier, inc=1, device_id=partner, device_id_type=pl.DeviceIdType.MESH)

    own_rows = aligned(sp * shard, shard, shard)

    def weight_loads():
        copies = []
        for j in range(tiles):
            for side, source in enumerate((gw_hbm, vw_hbm)):
                copies.append(
                    pltpu.make_async_copy(
                        source.at[:, pl.ds(j * LANES, LANES)],
                        wgv.at[own_rows, pl.ds((2 * j + side) * LANES, LANES)],
                        wload_sem.at[2 * j + side],
                    )
                )
        copies.append(pltpu.make_async_copy(dw_hbm, wd.at[own_rows, :], wload_sem.at[2 * tiles]))
        return copies

    mix_load = pltpu.make_async_copy(mix_hbm, mixb, load_sem.at[0])
    jump_loads = [
        pltpu.make_async_copy(
            jump_hbm.at[:, pl.ds(g * LANES, LANES)], a_s.at[g], load_sem.at[5 + g]
        )
        for g in range(groups)
    ]
    gate_load = pltpu.make_async_copy(gate_hbm, gateb, load_sem.at[1])
    outw_load = pltpu.make_async_copy(outw_hbm, outw, load_sem.at[2])
    resid_load = pltpu.make_async_copy(
        resid_hbm.at[aligned(t * rows, rows, 16), :], resid, load_sem.at[3]
    )
    mix_load.start()
    loads = weight_loads()
    for copy in loads:
        copy.start()
    for copy in jump_loads:
        copy.start()
    gate_load.start()
    outw_load.start()
    resid_load.start()
    for g in range(groups):
        maps[g, :, :LANES] = recur_map[g]
        maps[g, :, LANES:] = input_map[g]

    pl.semaphore_wait(barrier, len(partners))

    halo_copy = pltpu.make_async_remote_copy(
        src_ref=mix_hbm.at[pl.ds(length - 16, 16), :],
        dst_ref=halo,
        send_sem=halo_sem.at[0],
        recv_sem=halo_sem.at[1],
        device_id=sp_id(after),
        device_id_type=pl.DeviceIdType.MESH,
    )
    halo_copy.start()
    for copy in loads:
        copy.wait()

    near = 2 * (far - 1)
    gv_steps = near + 1
    d_steps = far
    steps = gv_steps + d_steps

    def piece(way, index):
        if index < gv_steps:
            distance, part = index // 2 + 1, index % 2
            if index == near:
                part = way
        else:
            distance, part = index - gv_steps + 1, None
        origin = lax.rem(chip + (chips - distance if way == 0 else distance), chips)
        return distance, part, origin

    def piece_ref(origin, part, way, distance):
        start = (2 * origin + core) * shard
        if part is not None:
            return wgv.at[aligned(start, shard, shard), pl.ds(part * width, width)]
        if distance == far:
            share = shard // 2
            return wd.at[aligned(start + way * share, share, share), :]
        return wd.at[aligned(start, shard, shard), :]

    def ring_copy(way, index):
        distance, part, _ = piece(way, index)
        source = distance - 1
        origin = lax.rem(chip + (chips - source if way == 0 else source), chips)
        ref = piece_ref(origin, part, way, distance)
        return pltpu.make_async_remote_copy(
            src_ref=ref,
            dst_ref=ref,
            send_sem=ring_send.at[way, index],
            recv_sem=ring_recv.at[way, index],
            device_id=sp_id(z_next[way]),
            device_id_type=pl.DeviceIdType.MESH,
        )

    def twin_copy(ref, kind):
        return pltpu.make_async_remote_copy(
            src_ref=ref,
            dst_ref=ref,
            send_sem=twin_send.at[kind],
            recv_sem=twin_recv.at[kind],
            device_id=sp_id(twin),
            device_id_type=pl.DeviceIdType.MESH,
        )

    def arrived(way, index):
        distance, part, origin = piece(way, index)
        ref = piece_ref(origin, part, way, distance)
        pltpu.make_async_remote_copy(
            src_ref=ref,
            dst_ref=ref,
            send_sem=ring_send.at[way, index],
            recv_sem=ring_recv.at[way, index],
            device_id=sp_id(z_next[way]),
            device_id_type=pl.DeviceIdType.MESH,
        ).wait_recv()
        if index < gv_steps:
            onward = index + 2
            if distance < far and (distance < far - 1 or part == way):
                onward = near if distance == far - 1 else onward
                ring_copy(way, onward).start()
        elif distance < far:
            ring_copy(way, index + 1).start()
        twin_copy(ref, 0 if index < gv_steps else 1).start()

    progress = [0]

    def pump(count):
        for _ in range(count):
            index = progress[0]
            if index >= steps:
                return
            if index == gv_steps - 2:
                for way in range(2):
                    ring_copy(way, gv_steps).start()
                twin_copy(piece_ref(chip, None, 0, 0), 1).start()
            for way in range(2):
                arrived(way, index)
            progress[0] = index + 1

    for index in range(2):
        for way in range(2):
            ring_copy(way, index).start()
    twin_copy(wgv.at[own_rows, :], 0).start()

    mix_load.wait()
    for g in range(groups):
        jump_loads[g].wait()
    xpad[pl.ds(8, length), :] = mixb[...].astype(jnp.float32)
    halo_copy.wait_recv()
    edge = halo[...].astype(jnp.float32)[8:, :]
    xpad[pl.ds(0, 8), :] = jnp.where(sp > 0, edge, 0.0)
    taps = mix_kernel[...].astype(jnp.float32)
    chunk = 64

    def gates(i):
        for g in range(groups):
            lanes = slice(g * LANES, (g + 1) * LANES)
            window = xpad[aligned(i * chunk, chunk + 8, 8), lanes]
            total = window[8:] * taps[3:4, lanes]
            for back in range(1, 4):
                total += pltpu.roll(window, back, 0)[8:] * taps[3 - back : 4 - back, lanes]
            conv = total.astype(jnp.bfloat16)
            both = jnp.dot(conv, maps[g], preferred_element_type=jnp.float32)
            at = aligned(i * chunk, chunk, 8)
            log_decay = sigmoid(both[:, :LANES]) * coef[:, lanes] + a_s[g, at, :]
            decay = jnp.exp(log_decay)
            loss = -jnp.tanh(log_decay) * (decay * decay + 1.0)
            drive = jnp.sqrt(loss) * sigmoid(both[:, LANES:]) * conv.astype(jnp.float32)
            a_s[g, at, :] = decay
            b_s[g, at, :] = drive

    pl.loop(0, length // chunk)(gates)
    pump(1)

    stretch = length // SEGMENTS

    def scan_step(i, carry):
        result = []
        for g in range(groups):
            product, state = carry[g]
            at = pl.ds(i, SEGMENTS, stride=stretch)
            decay = a_s[g, at, :]
            state = decay * state + b_s[g, at, :]
            product = product * decay
            a_s[g, at, :] = product
            b_s[g, at, :] = state
            result.append((product, state))
        return tuple(result)

    unit = jnp.ones((SEGMENTS, LANES), jnp.float32)
    ends = lax.fori_loop(0, stretch, scan_step, tuple((unit, unit * 0.0) for _ in range(groups)))
    segments = []
    for g in range(groups):
        product, state = ends[g]
        passed, held = unit[:1], unit[:1] * 0.0
        firsts, seconds = [], []
        for s in range(SEGMENTS):
            firsts.append(passed)
            seconds.append(held)
            held = product[s : s + 1] * held + state[s : s + 1]
            passed = passed * product[s : s + 1]
        segments.append((jnp.concatenate(firsts, axis=0), jnp.concatenate(seconds, axis=0)))
        own_ab[0:1, pl.ds(g * LANES, LANES)] = passed
        own_ab[1:2, pl.ds(g * LANES, LANES)] = held

    def team_copy(k):
        return pltpu.make_async_remote_copy(
            src_ref=own_ab,
            dst_ref=team_ab.at[TEAM - 1 - k],
            send_sem=team_send.at[k - 1],
            recv_sem=team_recv.at[k - 1],
            device_id=sp_id(mate(k)),
            device_id_type=pl.DeviceIdType.MESH,
        )

    def far_copy(k):
        return pltpu.make_async_remote_copy(
            src_ref=team_total,
            dst_ref=far_ab.at[k - 1],
            send_sem=far_send.at[k - 1],
            recv_sem=far_recv.at[k - 1],
            device_id=sp_id(far_mate(k)),
            device_id_type=pl.DeviceIdType.MESH,
        )

    for k in range(1, TEAM):
        team_copy(k).start()

    gate_load.wait()
    chunk2 = 176

    def gate_values(i):
        at = aligned(i * chunk2, chunk2, 16)
        for g in range(groups):
            gel[g, at, :] = gelu(gateb[at, g * LANES : (g + 1) * LANES].astype(jnp.float32))

    pl.loop(0, length // chunk2)(gate_values)

    for k in range(1, TEAM):
        team_copy(k).wait_recv()
    own = own_ab[...]
    head_a, head_b = jnp.ones_like(own[0:1]), jnp.zeros_like(own[0:1])
    tail_a, tail_b = own[0:1], own[1:2]
    for k in range(TEAM - 1, 0, -1):
        pair = team_ab[TEAM - 1 - k]
        inside = k <= place
        head_b = jnp.where(inside, pair[0:1] * head_b + pair[1:2], head_b)
        head_a = jnp.where(inside, pair[0:1] * head_a, head_a)
    for k in range(TEAM - 1, 0, -1):
        pair = team_ab[TEAM - 1 - k]
        behind = k > place
        tail_b = jnp.where(behind, pair[0:1] * tail_b + pair[1:2], tail_b)
        tail_a = jnp.where(behind, pair[0:1] * tail_a, tail_a)
    team_total[0:1, :] = head_a * tail_a
    team_total[1:2, :] = tail_a * head_b + tail_b
    for k in range(1, teams):
        far_copy(k).start()
    pump(2)
    for k in range(1, teams):
        far_copy(k).wait_recv()
    carried = jnp.zeros_like(own[0:1])
    for k in range(teams - 1, 0, -1):
        pair = far_ab[k - 1]
        carried = jnp.where(k <= team, pair[0:1] * carried + pair[1:2], carried)
    carried = head_a * carried + head_b

    inflow = [
        segments[g][0] * carried[:, g * LANES : (g + 1) * LANES] + segments[g][1]
        for g in range(groups)
    ]

    def finish_step(i):
        for g in range(groups):
            at = pl.ds(i, SEGMENTS, stride=stretch)
            state = a_s[g, at, :] * inflow[g] + b_s[g, at, :]
            b_s[g, at, :] = state * gel[g, at, :]

    pl.loop(0, stretch)(finish_step)
    for g in range(groups):
        branch[:, pl.ds(g * LANES, LANES)] = b_s[g].astype(jnp.bfloat16)
    outw_load.wait()
    pump(1)

    def reduce_scatter(partial, send, recv, ssem, rsem, finish, pumps):
        copies = []
        for s in range(num_tp):
            for q in range(2):
                for way in range(2):
                    shift = num_tp - 1 - s if way == 0 else 1 + s
                    block = lax.rem(t + shift, num_tp)
                    column = way * half + q * sub
                    value = partial(block, column)
                    if s > 0:
                        copies[4 * (s - 1) + 2 * q + way].wait_recv()
                        value = value + recv[way, s - 1, q].astype(jnp.float32)
                    if s < num_tp - 1:
                        send[way, s, q] = value.astype(jnp.bfloat16)
                        copy = pltpu.make_async_remote_copy(
                            src_ref=send.at[way, s, q],
                            dst_ref=recv.at[way, s, q],
                            send_sem=ssem.at[way, s, q],
                            recv_sem=rsem.at[way, s, q],
                            device_id=tp_id(t_next[way]),
                            device_id_type=pl.DeviceIdType.MESH,
                        )
                        copy.start()
                        copies.append(copy)
                    else:
                        finish(column, value)
                pump(pumps)
        return copies

    def mix_partial(block, column):
        return jnp.dot(
            branch[aligned(block * rows, rows, 16), :],
            outw[:, pl.ds(column, sub)],
            preferred_element_type=jnp.float32,
        )

    def keep_mixed(column, value):
        mixed[:, pl.ds(column, sub)] = value.astype(jnp.bfloat16)

    rs1_copies = reduce_scatter(
        mix_partial, rs1_send, rs1_recv, rs1_ssem, rs1_rsem, keep_mixed, 1
    )
    resid_load.wait()

    def scaled(value, gain):
        mean = jnp.mean(value * value, axis=-1, keepdims=True)
        return value * lax.rsqrt(mean + EPS) * gain[...]

    def norm_rows(i):
        at = aligned(i * 16, 16, 16)
        stream = resid[at, :].astype(jnp.float32)
        stream += scaled(mixed[at, :].astype(jnp.float32), mix_gain)
        stream = stream.astype(jnp.bfloat16)
        hidden[at, :] = stream
        normed[aligned(t * rows + i * 16, 16, 16), :] = scaled(
            stream.astype(jnp.float32), inner_gain
        ).astype(jnp.bfloat16)

    pl.loop(0, rows // 16)(norm_rows)

    order = ((0, 1, 2, 3), (2, 3, 0, 1))

    def gather_copy(way, index):
        source = 0 if index < 4 else 1
        block = lax.rem(t + (num_tp - source if way == 0 else source), num_tp)
        column = order[way][index % 4] * sub
        ref = normed.at[aligned(block * rows, rows, 16), pl.ds(column, sub)]
        return pltpu.make_async_remote_copy(
            src_ref=ref,
            dst_ref=ref,
            send_sem=ag_ssem.at[way, index],
            recv_sem=ag_rsem.at[way, index],
            device_id=tp_id(t_next[way]),
            device_id_type=pl.DeviceIdType.MESH,
        )

    def gather_wait(way, index):
        source = 1 if index < 4 else 2
        block = lax.rem(t + (num_tp - source if way == 0 else source), num_tp)
        column = order[way][index % 4] * sub
        ref = normed.at[aligned(block * rows, rows, 16), pl.ds(column, sub)]
        pltpu.make_async_remote_copy(
            src_ref=ref,
            dst_ref=ref,
            send_sem=ag_ssem.at[way, index],
            recv_sem=ag_rsem.at[way, index],
            device_id=tp_id(t_next[way]),
            device_id_type=pl.DeviceIdType.MESH,
        ).wait_recv()

    for index in range(4):
        for way in range(2):
            gather_copy(way, index).start()
    for index in range(2):
        for way in range(2):
            gather_wait(way, index)
            gather_copy(way, index + 4).start()
        pump(1)

    tail_copy = pltpu.make_async_remote_copy(
        src_ref=up.at[pl.ds(length, 16), :],
        dst_ref=up.at[pl.ds(0, 16), :],
        send_sem=tail_sem.at[0],
        recv_sem=tail_sem.at[1],
        device_id=sp_id(after),
        device_id_type=pl.DeviceIdType.MESH,
    )

    def up_block(block):
        source = aligned(block * rows, rows, 16)
        target = aligned(16 + block * rows, rows, 16)

        def tile(j):
            columns = aligned(j * 2 * LANES, 2 * LANES, LANES)
            up[target, columns] = jnp.dot(
                normed[source, :], wgv[:, columns], preferred_element_type=jnp.float32
            ).astype(jnp.bfloat16)

        pl.loop(0, tiles)(tile)

        @pl.when(block == num_tp - 1)
        def _():
            tail_copy.start()

    def act_block(block):
        @pl.when(block == 0)
        def _():
            tail_copy.wait_recv()

            @pl.when(sp == 0)
            def _():
                up[pl.ds(0, 16), :] = jnp.zeros((16, 2 * width), jnp.bfloat16)

        window = aligned(block * rows, rows + 16, 16)
        target = aligned(block * rows, rows, 16)

        def tile(j):
            columns = aligned(j * LANES, LANES, LANES)
            results = []
            for side, kernel in enumerate((gate_kernel, value_kernel)):
                start = (2 * j + side) * LANES
                value = up[window, aligned(start, LANES, LANES)].astype(jnp.float32)
                tap = kernel[:, columns].astype(jnp.float32)
                total = value[16:] * tap[2:3]
                for back in range(1, 3):
                    total += pltpu.roll(value, back, 0)[16:] * tap[2 - back : 3 - back]
                results.append(total)
            act[target, columns] = (gelu(results[0]) * results[1]).astype(jnp.bfloat16)

        pl.loop(0, tiles)(tile)

    def around(k):
        return lax.rem(t + k, num_tp)

    pump(gv_steps - progress[0])
    rival = wgv.at[pl.ds(0, chips * shard), :]
    pltpu.make_async_copy(rival, rival, twin_recv.at[0]).wait()
    up_block(around(0))
    pump(1)
    for index in range(2, 4):
        gather_wait(0, index)
    up_block(around(num_tp - 1))
    pump(1)
    for index in range(2, 4):
        gather_wait(1, index)
    up_block(around(1))
    pump(1)
    act_block(around(0))
    pump(1)
    act_block(around(1))
    pump(1)
    for index in range(4, 6):
        for way in range(2):
            gather_wait(way, index)
    up_block(around(2))
    pump(1)
    act_block(around(2))
    pump(1)
    act_block(around(num_tp - 1))
    pump(steps)
    rival = wd.at[pl.ds(0, chips * shard), :]
    pltpu.make_async_copy(rival, rival, twin_recv.at[1]).wait()

    def down_partial(block, column):
        return lax.dot_general(
            act[aligned(block * rows, rows, 16), :],
            wd[pl.ds(column, sub), :],
            (((1,), (1,)), ((), ())),
            preferred_element_type=jnp.float32,
        )

    rs2_copies = reduce_scatter(
        down_partial, rs2_send, rs2_recv, rs2_ssem, rs2_rsem, keep_mixed, 0
    )

    def last_rows(i):
        at = aligned(i * 16, 16, 16)
        stream = hidden[at, :].astype(jnp.float32)
        stream += scaled(mixed[at, :].astype(jnp.float32), final_gain)
        out_ref[at, :] = stream.astype(jnp.bfloat16)

    pl.loop(0, rows // 16)(last_rows)

    halo_copy.wait_send()
    tail_copy.wait_send()
    for k in range(1, TEAM):
        team_copy(k).wait_send()
    for k in range(1, teams):
        far_copy(k).wait_send()
    for index in range(steps):
        for way in range(2):
            ring_copy(way, index).wait_send()
    gathered = wgv.at[pl.ds(0, chips * shard), :]
    pltpu.make_async_copy(gathered, gathered, twin_send.at[0]).wait()
    gathered = wd.at[pl.ds(0, chips * shard), :]
    pltpu.make_async_copy(gathered, gathered, twin_send.at[1]).wait()
    for copy in rs1_copies + rs2_copies:
        copy.wait_send()
    for index in range(6):
        for way in range(2):
            gather_copy(way, index).wait_send()


def local(
    num_sp,
    num_tp,
    residual,
    mix_input,
    gate_input,
    mix_kernel,
    recur_gate_map,
    input_gate_map,
    decay_param,
    jump_log,
    out_weight,
    mix_gain,
    inner_gain,
    final_gain,
    gate_weight,
    value_weight,
    gate_kernel,
    value_kernel,
    down_weight,
):
    length, channels = mix_input.shape
    model = residual.shape[1]
    shard, width = gate_weight.shape
    rows = length // num_tp
    sub = model // 4
    groups = channels // LANES
    coef = (-GATE_SCALE * jax.nn.softplus(-decay_param)).reshape(1, channels)
    far = num_sp // 4
    steps = 2 * (far - 1) + 1 + far
    hbm = pl.BlockSpec(memory_space=pl.ANY)
    vmem = pl.BlockSpec(memory_space=pltpu.VMEM)
    bf16, f32 = jnp.bfloat16, jnp.float32
    dma = pltpu.SemaphoreType.DMA
    flow = (2, num_tp - 1, 2, rows, sub)
    return pl.pallas_call(
        functools.partial(layer_kernel, num_sp, num_tp),
        out_shape=jax.ShapeDtypeStruct((rows, model), bf16),
        in_specs=[hbm] * 8 + [vmem] * 9,
        out_specs=vmem,
        scratch_shapes=[
            pltpu.VMEM((num_sp * shard, 2 * width), bf16),
            pltpu.VMEM((num_sp * shard, width), bf16),
            pltpu.VMEM((length, channels), bf16),
            pltpu.VMEM((16, channels), bf16),
            pltpu.VMEM((length, channels), bf16),
            pltpu.VMEM((groups, length, LANES), f32),
            pltpu.VMEM((groups, length, LANES), f32),
            pltpu.VMEM((groups, length, LANES), f32),
            pltpu.VMEM((length + 8, channels), f32),
            pltpu.VMEM((groups, LANES, 2 * LANES), bf16),
            pltpu.VMEM((length, channels), bf16),
            pltpu.VMEM((channels, model), bf16),
            pltpu.VMEM((rows, model), bf16),
            pltpu.VMEM((2, channels), f32),
            pltpu.VMEM((TEAM - 1, 2, channels), f32),
            pltpu.VMEM((2, channels), f32),
            pltpu.VMEM((num_sp // TEAM - 1, 2, channels), f32),
            pltpu.VMEM(flow, bf16),
            pltpu.VMEM(flow, bf16),
            pltpu.VMEM(flow, bf16),
            pltpu.VMEM(flow, bf16),
            pltpu.VMEM((rows, model), bf16),
            pltpu.VMEM((rows, model), bf16),
            pltpu.VMEM((length, model), bf16),
            pltpu.VMEM((16 + length, 2 * width), bf16),
            pltpu.VMEM((length, width), bf16),
            dma((5 + groups,)),
            dma((2 * (width // LANES) + 1,)),
            dma((2,)),
            dma((2,)),
            dma((TEAM - 1,)),
            dma((TEAM - 1,)),
            dma((num_sp // TEAM - 1,)),
            dma((num_sp // TEAM - 1,)),
            dma((2, steps)),
            dma((2, steps)),
            dma((2,)),
            dma((2,)),
            dma(flow[:3]),
            dma(flow[:3]),
            dma(flow[:3]),
            dma(flow[:3]),
            dma((2, 6)),
            dma((2, 6)),
        ],
        compiler_params=pltpu.CompilerParams(
            collective_id=0, has_side_effects=True, vmem_limit_bytes=67043328
        ),
    )(
        mix_input,
        gate_input,
        jump_log,
        residual,
        out_weight,
        gate_weight,
        value_weight,
        down_weight.T,
        mix_kernel,
        recur_gate_map,
        input_gate_map,
        coef,
        mix_gain.reshape(1, model),
        inner_gain.reshape(1, model),
        final_gain.reshape(1, model),
        gate_kernel,
        value_kernel,
    )


def solution(mesh):
    return jax.shard_map(
        functools.partial(local, mesh.shape["sp"], mesh.shape["tp"]),
        mesh=mesh,
        in_specs=(
            P(("grp", "sp"), None),
            P(("grp", "sp"), "tp"),
            P(("grp", "sp"), "tp"),
            P(None, "tp"),
            P("tp", None, None),
            P("tp", None, None),
            P("tp"),
            P(("grp", "sp"), "tp"),
            P("tp", None),
            P(),
            P(),
            P(),
            P("sp", "tp"),
            P("sp", "tp"),
            P(None, "tp"),
            P(None, "tp"),
            P("tp", "sp"),
        ),
        out_specs=P(("grp", "sp", "tp"), None),
        check_vma=False,
    )
```

```python
import functools

import jax
import jax.numpy as jnp
from jax import lax
from jax.experimental import pallas as pl
from jax.experimental.pallas import tpu as pltpu
from jax.sharding import PartitionSpec as P

EPS = 1e-06
GATE_SCALE = 8.0
LANES = 128
SEGMENTS = 8
TEAM = 8
SQRT_2_PI = 0.7978845608028654


def gelu(v):
    return 0.5 * v * (1.0 + jnp.tanh(SQRT_2_PI * (v + 0.044715 * (v * v * v))))


def sigmoid(v):
    return 1.0 / (1.0 + jnp.exp(-v))


def softplus(v):
    z = jnp.exp(-jnp.abs(v))
    ratio = z / (2.0 + z)
    square = ratio * ratio
    series = jnp.full_like(square, 1.0 / 19.0)
    for power in range(17, 0, -2):
        series = series * square + 1.0 / power
    return jnp.maximum(v, 0.0) + 2.0 * ratio * series


def aligned(start, size, multiple):
    return pl.ds(pl.multiple_of(start, multiple), size)


def layer_kernel(
    num_sp,
    num_tp,
    mix_hbm,
    gate_hbm,
    jump_hbm,
    resid_hbm,
    outw_hbm,
    gw_hbm,
    vw_hbm,
    dw_hbm,
    mix_kernel,
    recur_map,
    input_map,
    decay_param,
    mix_gain,
    inner_gain,
    final_gain,
    gate_kernel,
    value_kernel,
    out_ref,
    wgv,
    wd,
    mixb,
    halo,
    gateb,
    a_s,
    b_s,
    gel,
    xpad,
    maps,
    branch,
    outw,
    resid,
    own_ab,
    team_ab,
    team_total,
    far_ab,
    rs1_send,
    rs1_recv,
    rs2_send,
    rs2_recv,
    mixed,
    hidden,
    normed,
    up,
    act,
    load_sem,
    wload_sem,
    halo_sem,
    tail_sem,
    team_send,
    team_recv,
    far_send,
    far_recv,
    ring_send,
    ring_recv,
    pair_send,
    pair_recv,
    twin_send,
    twin_recv,
    rs1_ssem,
    rs1_rsem,
    rs2_ssem,
    rs2_rsem,
    ag_ssem,
    ag_rsem,
):
    sp = lax.axis_index("sp")
    grp = lax.axis_index("grp")
    parity = lax.rem(grp, 2)
    pair_grp = grp + 1 - 2 * parity
    t = lax.axis_index("tp")
    length, channels = mixb.shape
    groups = channels // LANES
    shard = gw_hbm.shape[0]
    width = gw_hbm.shape[1]
    tiles = width // LANES
    model = outw.shape[1]
    rows = length // num_tp
    half = model // 2
    sub = half // 2
    chips = num_sp // 2
    far = chips // 2
    core = lax.rem(sp, 2)
    chip = sp // 2
    twin = sp + 1 - 2 * core
    after = lax.rem(sp + 1, num_sp)
    before = lax.rem(sp + num_sp - 1, num_sp)
    z_next = (lax.rem(sp + 2, num_sp), lax.rem(sp + num_sp - 2, num_sp))
    t_next = (lax.rem(t + 1, num_tp), lax.rem(t + num_tp - 1, num_tp))
    place = lax.rem(sp, TEAM)
    team = sp // TEAM
    teams = num_sp // TEAM

    def sp_id(index):
        return {"sp": index}

    def tp_id(index):
        return {"tp": index}

    def mate(k):
        return team * TEAM + lax.rem(place + k, TEAM)

    def far_mate(k):
        return lax.rem(sp + TEAM * k, num_sp)

    barrier = pltpu.get_barrier_semaphore()
    partners = [sp_id(after), sp_id(before), sp_id(z_next[0]), sp_id(z_next[1])]
    partners += [sp_id(mate(k)) for k in range(1, TEAM)]
    partners += [sp_id(far_mate(k)) for k in range(1, teams)]
    partners += [tp_id(lax.rem(t + k, num_tp)) for k in range(1, num_tp)]
    partners += [{"grp": pair_grp}]
    for partner in partners:
        pl.semaphore_signal(barrier, inc=1, device_id=partner, device_id_type=pl.DeviceIdType.MESH)

    own_rows = aligned(sp * shard, shard, shard)

    def weight_loads():
        copies = []
        for j in range(tiles):
            for side, source in enumerate((gw_hbm, vw_hbm)):
                copies.append(
                    pltpu.make_async_copy(
                        source.at[:, pl.ds(j * LANES, LANES)],
                        wgv.at[own_rows, pl.ds((2 * j + side) * LANES, LANES)],
                        wload_sem.at[2 * j + side],
                    )
                )
        copies.append(pltpu.make_async_copy(dw_hbm, wd.at[own_rows, :], wload_sem.at[2 * tiles]))
        return copies

    mix_load = pltpu.make_async_copy(mix_hbm, mixb, load_sem.at[0])
    jump_loads = [
        pltpu.make_async_copy(
            jump_hbm.at[:, pl.ds(g * LANES, LANES)], a_s.at[g], load_sem.at[5 + g]
        )
        for g in range(groups)
    ]
    gate_load = pltpu.make_async_copy(gate_hbm, gateb, load_sem.at[1])
    outw_load = pltpu.make_async_copy(outw_hbm, outw, load_sem.at[2])
    resid_load = pltpu.make_async_copy(
        resid_hbm.at[aligned(t * rows, rows, 16), :], resid, load_sem.at[3]
    )
    mix_load.start()
    loads = weight_loads()
    for copy in loads:
        copy.start()
    for copy in jump_loads:
        copy.start()
    gate_load.start()
    outw_load.start()
    resid_load.start()
    for g in range(groups):
        maps[g, :, :LANES] = recur_map[g]
        maps[g, :, LANES:] = input_map[g]

    whole = (wgv, wd)
    lone = ((2 * tiles // 3) * LANES, ((tiles + 1) // 3) * LANES)
    near = 2 * (far - 1)
    per_stage = near + 1

    def part_ref(stage, origin, part, side):
        ref, size = whole[stage], lone[stage]
        at = aligned((2 * origin + core) * shard, shard, shard)
        if part == 0:
            return ref.at[at, aligned(side * size, size, LANES)]
        return ref.at[at, pl.ds(2 * size, ref.shape[1] - 2 * size)]

    def origin_at(way, distance):
        return lax.rem(chip + (chips - distance if way == 0 else distance), chips)

    def what(way, index):
        return index // 2 + 1, (way if index == near else index % 2)

    def remote(ref, send_sem, recv_sem, device_id):
        return pltpu.make_async_remote_copy(
            src_ref=ref,
            dst_ref=ref,
            send_sem=send_sem,
            recv_sem=recv_sem,
            device_id=device_id,
            device_id_type=pl.DeviceIdType.MESH,
        )

    def ring_copy(way, stage, index, received=False):
        distance, part = what(way, index)
        ref = part_ref(stage, origin_at(way, distance - (0 if received else 1)), part, parity)
        slot = stage * per_stage + index
        return remote(
            ref, ring_send.at[way, slot], ring_recv.at[way, slot], sp_id(z_next[way])
        )

    def pair_copy(way, stage, distance, received=False):
        side = 1 - parity if received else parity
        ref = part_ref(stage, origin_at(way, distance), 0, side)
        slot = stage * per_stage + way * far + distance - 1
        return remote(ref, pair_send.at[slot], pair_recv.at[slot], {"grp": pair_grp})

    def twin_copy(ref, stage):
        return remote(ref, twin_send.at[stage], twin_recv.at[stage], sp_id(twin))

    def arrived(way, stage, index):
        distance, part = what(way, index)
        ring_copy(way, stage, index, True).wait_recv()
        if distance < far - 1:
            ring_copy(way, stage, index + 2).start()
        elif distance == far - 1 and part == way:
            ring_copy(way, stage, near).start()
        if part == 0:
            pair_copy(way, stage, distance).start()
        twin_copy(part_ref(stage, origin_at(way, distance), part, parity), stage).start()

    def crossed(way, stage, distance):
        pair_copy(way, stage, distance, True).wait_recv()
        twin_copy(part_ref(stage, origin_at(way, distance), 0, 1 - parity), stage).start()

    def ring_start(stage, part):
        for way in range(2):
            ring_copy(way, stage, part).start()

    def event(stage, index):
        if index < per_stage:
            for way in range(2):
                arrived(way, stage, index)
            if index % 2 == 1 and index > 1:
                for way in range(2):
                    crossed(way, stage, (index - 1) // 2)
        else:
            for way in range(2):
                crossed(way, stage, far - 1)
            crossed(0, stage, far)

    events = [(0, k) for k in range(per_stage)] + [(1, 0), (0, per_stage)]
    first_done = len(events)
    events += [(1, k) for k in range(1, per_stage + 1)]
    progress = [0]

    def pump(count):
        for _ in range(count):
            number = progress[0]
            if number >= len(events):
                return
            if number == per_stage - 2:
                ring_start(1, 0)
                ring_start(1, 1)
                twin_copy(wd.at[own_rows, :], 1).start()
            event(*events[number])
            progress[0] = number + 1

    mix_load.wait()
    for g in range(groups):
        jump_loads[g].wait()
    xpad[pl.ds(8, length), :] = mixb[...].astype(jnp.float32)
    taps = mix_kernel[...].astype(jnp.float32)
    coef = -GATE_SCALE * softplus(-decay_param[...])
    chunk = 64

    def gates(i):
        for g in range(groups):
            lanes = slice(g * LANES, (g + 1) * LANES)
            window = xpad[aligned(i * chunk, chunk + 8, 8), lanes]
            total = window[8:] * taps[3:4, lanes]
            for back in range(1, 4):
                total += pltpu.roll(window, back, 0)[8:] * taps[3 - back : 4 - back, lanes]
            conv = total.astype(jnp.bfloat16)
            both = jnp.dot(conv, maps[g], preferred_element_type=jnp.float32)
            at = aligned(i * chunk, chunk, 8)
            log_decay = sigmoid(both[:, :LANES]) * coef[:, lanes] + a_s[g, at, :]
            decay = jnp.exp(log_decay)
            loss = -jnp.tanh(log_decay) * (decay * decay + 1.0)
            drive = jnp.sqrt(loss) * sigmoid(both[:, LANES:]) * conv.astype(jnp.float32)
            a_s[g, at, :] = decay
            b_s[g, at, :] = drive

    pl.loop(1, length // chunk)(gates)
    gate_load.wait()
    chunk2 = 176

    def gate_values(i):
        at = aligned(i * chunk2, chunk2, 16)
        for g in range(groups):
            gel[g, at, :] = gelu(gateb[at, g * LANES : (g + 1) * LANES].astype(jnp.float32))

    pl.semaphore_wait(barrier, len(partners))

    halo_copy = pltpu.make_async_remote_copy(
        src_ref=mix_hbm.at[pl.ds(length - 16, 16), :],
        dst_ref=halo,
        send_sem=halo_sem.at[0],
        recv_sem=halo_sem.at[1],
        device_id=sp_id(after),
        device_id_type=pl.DeviceIdType.MESH,
    )
    halo_copy.start()
    pl.loop(0, length // chunk2)(gate_values)
    for copy in loads:
        copy.wait()
    halo_copy.wait_recv()
    edge = halo[...].astype(jnp.float32)[8:, :]
    xpad[pl.ds(0, 8), :] = jnp.where(sp > 0, edge, 0.0)
    gates(0)

    stretch = length // SEGMENTS

    def scan_step(i, carry):
        result = []
        for g in range(groups):
            product, state = carry[g]
            at = pl.ds(i, SEGMENTS, stride=stretch)
            decay = a_s[g, at, :]
            state = decay * state + b_s[g, at, :]
            product = product * decay
            a_s[g, at, :] = product
            b_s[g, at, :] = state
            result.append((product, state))
        return tuple(result)

    unit = jnp.ones((SEGMENTS, LANES), jnp.float32)
    ends = lax.fori_loop(0, stretch, scan_step, tuple((unit, unit * 0.0) for _ in range(groups)))
    segments = []
    for g in range(groups):
        product, state = ends[g]
        passed, held = unit[:1], unit[:1] * 0.0
        firsts, seconds = [], []
        for s in range(SEGMENTS):
            firsts.append(passed)
            seconds.append(held)
            held = product[s : s + 1] * held + state[s : s + 1]
            passed = passed * product[s : s + 1]
        segments.append((jnp.concatenate(firsts, axis=0), jnp.concatenate(seconds, axis=0)))
        own_ab[0:1, pl.ds(g * LANES, LANES)] = passed
        own_ab[1:2, pl.ds(g * LANES, LANES)] = held

    def team_copy(k):
        return pltpu.make_async_remote_copy(
            src_ref=own_ab,
            dst_ref=team_ab.at[TEAM - 1 - k],
            send_sem=team_send.at[k - 1],
            recv_sem=team_recv.at[k - 1],
            device_id=sp_id(mate(k)),
            device_id_type=pl.DeviceIdType.MESH,
        )

    def far_copy(k):
        return pltpu.make_async_remote_copy(
            src_ref=team_total,
            dst_ref=far_ab.at[k - 1],
            send_sem=far_send.at[k - 1],
            recv_sem=far_recv.at[k - 1],
            device_id=sp_id(far_mate(k)),
            device_id_type=pl.DeviceIdType.MESH,
        )

    for k in range(1, TEAM):
        team_copy(k).start()
    ring_start(0, 0)
    twin_copy(wgv.at[own_rows, :], 0).start()

    for k in range(1, TEAM):
        team_copy(k).wait_recv()
    own = own_ab[...]
    head_a, head_b = jnp.ones_like(own[0:1]), jnp.zeros_like(own[0:1])
    tail_a, tail_b = own[0:1], own[1:2]
    for k in range(TEAM - 1, 0, -1):
        pair = team_ab[TEAM - 1 - k]
        inside = k <= place
        head_b = jnp.where(inside, pair[0:1] * head_b + pair[1:2], head_b)
        head_a = jnp.where(inside, pair[0:1] * head_a, head_a)
    for k in range(TEAM - 1, 0, -1):
        pair = team_ab[TEAM - 1 - k]
        behind = k > place
        tail_b = jnp.where(behind, pair[0:1] * tail_b + pair[1:2], tail_b)
        tail_a = jnp.where(behind, pair[0:1] * tail_a, tail_a)
    team_total[0:1, :] = head_a * tail_a
    team_total[1:2, :] = tail_a * head_b + tail_b
    for k in range(1, teams):
        far_copy(k).start()
    ring_start(0, 1)
    pump(2)
    for k in range(1, teams):
        far_copy(k).wait_recv()
    carried = jnp.zeros_like(own[0:1])
    for k in range(teams - 1, 0, -1):
        pair = far_ab[k - 1]
        carried = jnp.where(k <= team, pair[0:1] * carried + pair[1:2], carried)
    carried = head_a * carried + head_b

    inflow = [
        segments[g][0] * carried[:, g * LANES : (g + 1) * LANES] + segments[g][1]
        for g in range(groups)
    ]

    def finish_step(i):
        for g in range(groups):
            at = pl.ds(i, SEGMENTS, stride=stretch)
            state = a_s[g, at, :] * inflow[g] + b_s[g, at, :]
            b_s[g, at, :] = state * gel[g, at, :]

    pl.loop(0, stretch)(finish_step)
    for g in range(groups):
        branch[:, pl.ds(g * LANES, LANES)] = b_s[g].astype(jnp.bfloat16)
    outw_load.wait()
    pump(1)

    def reduce_scatter(partial, send, recv, ssem, rsem, finish, pumps):
        copies = []
        for s in range(num_tp):
            for q in range(2):
                for way in range(2):
                    shift = num_tp - 1 - s if way == 0 else 1 + s
                    block = lax.rem(t + shift, num_tp)
                    column = way * half + q * sub
                    value = partial(block, column)
                    if s > 0:
                        copies[4 * (s - 1) + 2 * q + way].wait_recv()
                        value = value + recv[way, s - 1, q].astype(jnp.float32)
                    if s < num_tp - 1:
                        send[way, s, q] = value.astype(jnp.bfloat16)
                        copy = pltpu.make_async_remote_copy(
                            src_ref=send.at[way, s, q],
                            dst_ref=recv.at[way, s, q],
                            send_sem=ssem.at[way, s, q],
                            recv_sem=rsem.at[way, s, q],
                            device_id=tp_id(t_next[way]),
                            device_id_type=pl.DeviceIdType.MESH,
                        )
                        copy.start()
                        copies.append(copy)
                    else:
                        finish(column, value)
                pump(pumps[2 * s + q])
        return copies

    def mix_partial(block, column):
        return jnp.dot(
            branch[aligned(block * rows, rows, 16), :],
            outw[:, pl.ds(column, sub)],
            preferred_element_type=jnp.float32,
        )

    def keep_mixed(column, value):
        mixed[:, pl.ds(column, sub)] = value.astype(jnp.bfloat16)

    rs1_copies = reduce_scatter(
        mix_partial, rs1_send, rs1_recv, rs1_ssem, rs1_rsem, keep_mixed, (1, 1, 2, 1, 2, 1, 1, 1)
    )
    resid_load.wait()

    def scaled(value, gain):
        mean = jnp.mean(value * value, axis=-1, keepdims=True)
        return value * lax.rsqrt(mean + EPS) * gain[...]

    def norm_rows(i):
        at = aligned(i * 16, 16, 16)
        stream = resid[at, :].astype(jnp.float32)
        stream += scaled(mixed[at, :].astype(jnp.float32), mix_gain)
        stream = stream.astype(jnp.bfloat16)
        hidden[at, :] = stream
        normed[aligned(t * rows + i * 16, 16, 16), :] = scaled(
            stream.astype(jnp.float32), inner_gain
        ).astype(jnp.bfloat16)

    pl.loop(0, rows // 16)(norm_rows)

    order = ((0, 1, 2, 3), (2, 3, 0, 1))

    def gather_copy(way, index):
        source = 0 if index < 4 else 1
        block = lax.rem(t + (num_tp - source if way == 0 else source), num_tp)
        column = order[way][index % 4] * sub
        ref = normed.at[aligned(block * rows, rows, 16), pl.ds(column, sub)]
        return pltpu.make_async_remote_copy(
            src_ref=ref,
            dst_ref=ref,
            send_sem=ag_ssem.at[way, index],
            recv_sem=ag_rsem.at[way, index],
            device_id=tp_id(t_next[way]),
            device_id_type=pl.DeviceIdType.MESH,
        )

    def gather_wait(way, index):
        source = 1 if index < 4 else 2
        block = lax.rem(t + (num_tp - source if way == 0 else source), num_tp)
        column = order[way][index % 4] * sub
        ref = normed.at[aligned(block * rows, rows, 16), pl.ds(column, sub)]
        pltpu.make_async_remote_copy(
            src_ref=ref,
            dst_ref=ref,
            send_sem=ag_ssem.at[way, index],
            recv_sem=ag_rsem.at[way, index],
            device_id=tp_id(t_next[way]),
            device_id_type=pl.DeviceIdType.MESH,
        ).wait_recv()

    for index in range(4):
        for way in range(2):
            gather_copy(way, index).start()
    for index in range(2):
        pump(2)
        for way in range(2):
            gather_wait(way, index)
            gather_copy(way, index + 4).start()

    tail_copy = pltpu.make_async_remote_copy(
        src_ref=up.at[pl.ds(length, 16), :],
        dst_ref=up.at[pl.ds(0, 16), :],
        send_sem=tail_sem.at[0],
        recv_sem=tail_sem.at[1],
        device_id=sp_id(after),
        device_id_type=pl.DeviceIdType.MESH,
    )

    def up_block(block):
        source = aligned(block * rows, rows, 16)
        target = aligned(16 + block * rows, rows, 16)

        def tile(j):
            columns = aligned(j * 2 * LANES, 2 * LANES, LANES)
            up[target, columns] = jnp.dot(
                normed[source, :], wgv[:, columns], preferred_element_type=jnp.float32
            ).astype(jnp.bfloat16)

        pl.loop(0, tiles)(tile)

        @pl.when(block == num_tp - 1)
        def _():
            tail_copy.start()

    def act_block(block):
        @pl.when(block == 0)
        def _():
            tail_copy.wait_recv()

            @pl.when(sp == 0)
            def _():
                up[pl.ds(0, 16), :] = jnp.zeros((16, 2 * width), jnp.bfloat16)

        window = aligned(block * rows, rows + 16, 16)
        target = aligned(block * rows, rows, 16)

        def tile(j):
            columns = aligned(j * LANES, LANES, LANES)
            results = []
            for side, kernel in enumerate((gate_kernel, value_kernel)):
                start = (2 * j + side) * LANES
                value = up[window, aligned(start, LANES, LANES)].astype(jnp.float32)
                tap = kernel[:, columns].astype(jnp.float32)
                total = value[16:] * tap[2:3]
                for back in range(1, 3):
                    total += pltpu.roll(value, back, 0)[16:] * tap[2 - back : 3 - back]
                results.append(total)
            act[target, columns] = (gelu(results[0]) * results[1]).astype(jnp.bfloat16)

        pl.loop(0, tiles)(tile)

    def around(k):
        return lax.rem(t + k, num_tp)

    pump(first_done - progress[0])
    rival = wgv.at[pl.ds(0, chips * shard), :]
    pltpu.make_async_copy(rival, rival, twin_recv.at[0]).wait()
    up_block(around(0))
    pump(2)
    for index in range(2, 4):
        gather_wait(0, index)
    up_block(around(num_tp - 1))
    pump(2)
    for index in range(2, 4):
        gather_wait(1, index)
    up_block(around(1))
    pump(2)
    act_block(around(0))
    pump(2)
    act_block(around(1))
    pump(2)
    for index in range(4, 6):
        for way in range(2):
            gather_wait(way, index)
    up_block(around(2))
    pump(2)
    act_block(around(2))
    pump(2)
    act_block(around(num_tp - 1))
    pump(len(events))
    rival = wd.at[pl.ds(0, chips * shard), :]
    pltpu.make_async_copy(rival, rival, twin_recv.at[1]).wait()

    def down_partial(block, column):
        return lax.dot_general(
            act[aligned(block * rows, rows, 16), :],
            wd[pl.ds(column, sub), :],
            (((1,), (1,)), ((), ())),
            preferred_element_type=jnp.float32,
        )

    rs2_copies = reduce_scatter(
        down_partial, rs2_send, rs2_recv, rs2_ssem, rs2_rsem, keep_mixed, (0,) * 8
    )

    def last_rows(i):
        at = aligned(i * 16, 16, 16)
        stream = hidden[at, :].astype(jnp.float32)
        stream += scaled(mixed[at, :].astype(jnp.float32), final_gain)
        out_ref[at, :] = stream.astype(jnp.bfloat16)

    pl.loop(0, rows // 16)(last_rows)

    halo_copy.wait_send()
    tail_copy.wait_send()
    for k in range(1, TEAM):
        team_copy(k).wait_send()
    for k in range(1, teams):
        far_copy(k).wait_send()
    for stage in range(2):
        for way in range(2):
            for index in range(per_stage):
                ring_copy(way, stage, index).wait_send()
            for distance in range(1, far + 1 - way):
                pair_copy(way, stage, distance).wait_send()
    gathered = wgv.at[pl.ds(0, chips * shard), :]
    pltpu.make_async_copy(gathered, gathered, twin_send.at[0]).wait()
    gathered = wd.at[pl.ds(0, chips * shard), :]
    pltpu.make_async_copy(gathered, gathered, twin_send.at[1]).wait()
    for copy in rs1_copies + rs2_copies:
        copy.wait_send()
    for index in range(6):
        for way in range(2):
            gather_copy(way, index).wait_send()


def local(
    num_sp,
    num_tp,
    residual,
    mix_input,
    gate_input,
    mix_kernel,
    recur_gate_map,
    input_gate_map,
    decay_param,
    jump_log,
    out_weight,
    mix_gain,
    inner_gain,
    final_gain,
    gate_weight,
    value_weight,
    gate_kernel,
    value_kernel,
    down_weight,
):
    length, channels = mix_input.shape
    model = residual.shape[1]
    shard, width = gate_weight.shape
    rows = length // num_tp
    sub = model // 4
    groups = channels // LANES
    far = num_sp // 4
    steps = 2 * (2 * far - 1)
    hbm = pl.BlockSpec(memory_space=pl.ANY)
    vmem = pl.BlockSpec(memory_space=pltpu.VMEM)
    bf16, f32 = jnp.bfloat16, jnp.float32
    dma = pltpu.SemaphoreType.DMA
    flow = (2, num_tp - 1, 2, rows, sub)
    return pl.pallas_call(
        functools.partial(layer_kernel, num_sp, num_tp),
        out_shape=jax.ShapeDtypeStruct((rows, model), bf16),
        in_specs=[hbm] * 8 + [vmem] * 9,
        out_specs=vmem,
        scratch_shapes=[
            pltpu.VMEM((num_sp * shard, 2 * width), bf16),
            pltpu.VMEM((num_sp * shard, width), bf16),
            pltpu.VMEM((length, channels), bf16),
            pltpu.VMEM((16, channels), bf16),
            pltpu.VMEM((length, channels), bf16),
            pltpu.VMEM((groups, length, LANES), f32),
            pltpu.VMEM((groups, length, LANES), f32),
            pltpu.VMEM((groups, length, LANES), f32),
            pltpu.VMEM((length + 8, channels), f32),
            pltpu.VMEM((groups, LANES, 2 * LANES), bf16),
            pltpu.VMEM((length, channels), bf16),
            pltpu.VMEM((channels, model), bf16),
            pltpu.VMEM((rows, model), bf16),
            pltpu.VMEM((2, channels), f32),
            pltpu.VMEM((TEAM - 1, 2, channels), f32),
            pltpu.VMEM((2, channels), f32),
            pltpu.VMEM((num_sp // TEAM - 1, 2, channels), f32),
            pltpu.VMEM(flow, bf16),
            pltpu.VMEM(flow, bf16),
            pltpu.VMEM(flow, bf16),
            pltpu.VMEM(flow, bf16),
            pltpu.VMEM((rows, model), bf16),
            pltpu.VMEM((rows, model), bf16),
            pltpu.VMEM((length, model), bf16),
            pltpu.VMEM((16 + length, 2 * width), bf16),
            pltpu.VMEM((length, width), bf16),
            dma((5 + groups,)),
            dma((2 * (width // LANES) + 1,)),
            dma((2,)),
            dma((2,)),
            dma((TEAM - 1,)),
            dma((TEAM - 1,)),
            dma((num_sp // TEAM - 1,)),
            dma((num_sp // TEAM - 1,)),
            dma((2, steps)),
            dma((2, steps)),
            dma((steps,)),
            dma((steps,)),
            dma((2,)),
            dma((2,)),
            dma(flow[:3]),
            dma(flow[:3]),
            dma(flow[:3]),
            dma(flow[:3]),
            dma((2, 6)),
            dma((2, 6)),
        ],
        compiler_params=pltpu.CompilerParams(
            collective_id=0, has_side_effects=True, vmem_limit_bytes=67043328
        ),
    )(
        mix_input,
        gate_input,
        jump_log,
        residual,
        out_weight,
        gate_weight,
        value_weight,
        down_weight.T,
        mix_kernel,
        recur_gate_map,
        input_gate_map,
        decay_param.reshape(1, channels),
        mix_gain.reshape(1, model),
        inner_gain.reshape(1, model),
        final_gain.reshape(1, model),
        gate_kernel,
        value_kernel,
    )


def solution(mesh):
    return jax.shard_map(
        functools.partial(local, mesh.shape["sp"], mesh.shape["tp"]),
        mesh=mesh,
        in_specs=(
            P(("grp", "sp"), None),
            P(("grp", "sp"), "tp"),
            P(("grp", "sp"), "tp"),
            P(None, "tp"),
            P("tp", None, None),
            P("tp", None, None),
            P("tp"),
            P(("grp", "sp"), "tp"),
            P("tp", None),
            P(),
            P(),
            P(),
            P("sp", "tp"),
            P("sp", "tp"),
            P(None, "tp"),
            P(None, "tp"),
            P("tp", "sp"),
        ),
        out_specs=P(("grp", "sp", "tp"), None),
        check_vma=False,
    )
```

```python
import functools

import jax
import jax.numpy as jnp
from jax import lax
from jax.experimental import pallas as pl
from jax.experimental.pallas import tpu as pltpu
from jax.sharding import PartitionSpec as P

EPS = 1e-06
GATE_SCALE = 8.0
LANES = 128
SEGMENTS = 8
TEAM = 8
SQRT_2_PI = 0.7978845608028654


def gelu(v):
    return 0.5 * v * (1.0 + jnp.tanh(SQRT_2_PI * (v + 0.044715 * (v * v * v))))


def sigmoid(v):
    return 1.0 / (1.0 + jnp.exp(-v))


def softplus(v):
    z = jnp.exp(-jnp.abs(v))
    ratio = z / (2.0 + z)
    square = ratio * ratio
    series = jnp.full_like(square, 1.0 / 19.0)
    for power in range(17, 0, -2):
        series = series * square + 1.0 / power
    return jnp.maximum(v, 0.0) + 2.0 * ratio * series


def aligned(start, size, multiple):
    return pl.ds(pl.multiple_of(start, multiple), size)


def layer_kernel(
    num_sp,
    num_tp,
    mix_hbm,
    gate_hbm,
    jump_hbm,
    resid_hbm,
    outw_hbm,
    gw_hbm,
    vw_hbm,
    dw_hbm,
    mix_kernel,
    recur_map,
    input_map,
    decay_param,
    mix_gain,
    inner_gain,
    final_gain,
    gate_kernel,
    value_kernel,
    out_ref,
    wgv,
    wd,
    mixb,
    halo,
    gateb,
    a_s,
    b_s,
    gel,
    xpad,
    maps,
    branch,
    outw,
    resid,
    own_ab,
    team_ab,
    team_total,
    far_ab,
    reached,
    rs1_send,
    rs1_recv,
    rs2_send,
    rs2_recv,
    mixed,
    hidden,
    normed,
    up,
    act,
    load_sem,
    wload_sem,
    halo_sem,
    tail_sem,
    team_send,
    team_recv,
    far_send,
    far_recv,
    ring_send,
    ring_recv,
    pair_send,
    pair_recv,
    twin_send,
    twin_recv,
    rs1_ssem,
    rs1_rsem,
    rs2_ssem,
    rs2_rsem,
    ag_ssem,
    ag_rsem,
):
    sp = lax.axis_index("sp")
    grp = lax.axis_index("grp")
    parity = lax.rem(grp, 2)
    pair_grp = grp + 1 - 2 * parity
    t = lax.axis_index("tp")
    length, channels = mixb.shape
    groups = channels // LANES
    shard = gw_hbm.shape[0]
    width = gw_hbm.shape[1]
    tiles = width // LANES
    model = outw.shape[1]
    rows = length // num_tp
    half = model // 2
    sub = half // 2
    chips = num_sp // 2
    far = chips // 2
    core = lax.rem(sp, 2)
    chip = sp // 2
    twin = sp + 1 - 2 * core
    after = lax.rem(sp + 1, num_sp)
    before = lax.rem(sp + num_sp - 1, num_sp)
    z_next = (lax.rem(sp + 2, num_sp), lax.rem(sp + num_sp - 2, num_sp))
    t_next = (lax.rem(t + 1, num_tp), lax.rem(t + num_tp - 1, num_tp))
    place = lax.rem(sp, TEAM)
    team = sp // TEAM
    teams = num_sp // TEAM

    def sp_id(index):
        return {"sp": index}

    def tp_id(index):
        return {"tp": index}

    def mate(k):
        return team * TEAM + lax.rem(place + k, TEAM)

    def far_mate(k):
        return lax.rem(sp + TEAM * k, num_sp)

    barrier = pltpu.get_barrier_semaphore()
    partners = [sp_id(after), sp_id(before), sp_id(z_next[0]), sp_id(z_next[1])]
    partners += [sp_id(mate(k)) for k in range(1, TEAM)]
    partners += [sp_id(far_mate(k)) for k in range(1, teams)]
    partners += [tp_id(lax.rem(t + k, num_tp)) for k in range(1, num_tp)]
    partners += [{"grp": pair_grp}]
    for partner in partners:
        pl.semaphore_signal(barrier, inc=1, device_id=partner, device_id_type=pl.DeviceIdType.MESH)

    own_rows = aligned(sp * shard, shard, shard)

    def weight_loads():
        copies = []
        for j in range(tiles):
            for side, source in enumerate((gw_hbm, vw_hbm)):
                copies.append(
                    pltpu.make_async_copy(
                        source.at[:, pl.ds(j * LANES, LANES)],
                        wgv.at[own_rows, pl.ds((2 * j + side) * LANES, LANES)],
                        wload_sem.at[2 * j + side],
                    )
                )
        copies.append(pltpu.make_async_copy(dw_hbm, wd.at[own_rows, :], wload_sem.at[2 * tiles]))
        return copies

    mix_load = pltpu.make_async_copy(mix_hbm, mixb, load_sem.at[0])
    jump_loads = [
        pltpu.make_async_copy(
            jump_hbm.at[:, pl.ds(g * LANES, LANES)], a_s.at[g], load_sem.at[5 + g]
        )
        for g in range(groups)
    ]
    gate_load = pltpu.make_async_copy(gate_hbm, gateb, load_sem.at[1])
    outw_load = pltpu.make_async_copy(outw_hbm, outw, load_sem.at[2])
    resid_load = pltpu.make_async_copy(
        resid_hbm.at[aligned(t * rows, rows, 16), :], resid, load_sem.at[3]
    )
    mix_load.start()
    loads = weight_loads()
    for copy in loads:
        copy.start()
    for copy in jump_loads:
        copy.start()
    gate_load.start()
    outw_load.start()
    resid_load.start()
    for g in range(groups):
        maps[g, :, :LANES] = recur_map[g]
        maps[g, :, LANES:] = input_map[g]

    whole = (wgv, wd)
    lone = ((2 * tiles // 3) * LANES, ((tiles + 1) // 3) * LANES)
    near = 2 * (far - 1)
    per_stage = near + 1

    def part_ref(stage, origin, part, side):
        ref, size = whole[stage], lone[stage]
        at = aligned((2 * origin + core) * shard, shard, shard)
        if part == 0:
            return ref.at[at, aligned(side * size, size, LANES)]
        return ref.at[at, pl.ds(2 * size, ref.shape[1] - 2 * size)]

    def origin_at(way, distance):
        return lax.rem(chip + (chips - distance if way == 0 else distance), chips)

    def what(way, index):
        return index // 2 + 1, (way if index == near else index % 2)

    def remote(ref, send_sem, recv_sem, device_id):
        return pltpu.make_async_remote_copy(
            src_ref=ref,
            dst_ref=ref,
            send_sem=send_sem,
            recv_sem=recv_sem,
            device_id=device_id,
            device_id_type=pl.DeviceIdType.MESH,
        )

    def ring_copy(way, stage, index, received=False):
        distance, part = what(way, index)
        ref = part_ref(stage, origin_at(way, distance - (0 if received else 1)), part, parity)
        slot = stage * per_stage + index
        return remote(
            ref, ring_send.at[way, slot], ring_recv.at[way, slot], sp_id(z_next[way])
        )

    def pair_copy(way, stage, distance, received=False):
        side = 1 - parity if received else parity
        ref = part_ref(stage, origin_at(way, distance), 0, side)
        slot = stage * per_stage + way * far + distance - 1
        return remote(ref, pair_send.at[slot], pair_recv.at[slot], {"grp": pair_grp})

    def twin_copy(ref, stage):
        return remote(ref, twin_send.at[stage], twin_recv.at[stage], sp_id(twin))

    def arrived(way, stage, index):
        distance, part = what(way, index)
        ring_copy(way, stage, index, True).wait_recv()
        if distance < far - 1:
            ring_copy(way, stage, index + 2).start()
        elif distance == far - 1 and part == way:
            ring_copy(way, stage, near).start()
        if part == 0:
            pair_copy(way, stage, distance).start()
        twin_copy(part_ref(stage, origin_at(way, distance), part, parity), stage).start()

    def crossed(way, stage, distance):
        pair_copy(way, stage, distance, True).wait_recv()
        twin_copy(part_ref(stage, origin_at(way, distance), 0, 1 - parity), stage).start()

    def ring_start(stage, part):
        for way in range(2):
            ring_copy(way, stage, part).start()

    def event(stage, index):
        if index < per_stage:
            for way in range(2):
                arrived(way, stage, index)
            if index % 2 == 1 and index > 1:
                for way in range(2):
                    crossed(way, stage, (index - 1) // 2)
        else:
            for way in range(2):
                crossed(way, stage, far - 1)
            crossed(0, stage, far)

    def at_distance(stage, distance):
        first = 2 * (distance - 1)
        return [(stage, k) for k in range(first, min(first + 2, per_stage))]

    lag = far // 2
    events = []
    for distance in range(1, far + 1):
        events += at_distance(0, distance)
        if distance > lag:
            events += at_distance(1, distance - lag)
        if distance == lag:
            down_start = len(events)
    events.append((0, per_stage))
    first_done = len(events)
    for distance in range(far - lag + 1, far + 1):
        events += at_distance(1, distance)
    events.append((1, per_stage))
    progress = [0]

    def pump(count):
        for _ in range(count):
            number = progress[0]
            if number >= len(events):
                return
            if number == down_start:
                ring_start(1, 0)
                ring_start(1, 1)
                twin_copy(wd.at[own_rows, :], 1).start()
            event(*events[number])
            progress[0] = number + 1

    mix_load.wait()
    for g in range(groups):
        jump_loads[g].wait()
    xpad[pl.ds(8, length), :] = mixb[...].astype(jnp.float32)
    taps = mix_kernel[...].astype(jnp.float32)
    coef = -GATE_SCALE * softplus(-decay_param[...])
    chunk = 64

    def gates(i):
        for g in range(groups):
            lanes = slice(g * LANES, (g + 1) * LANES)
            window = xpad[aligned(i * chunk, chunk + 8, 8), lanes]
            total = window[8:] * taps[3:4, lanes]
            for back in range(1, 4):
                total += pltpu.roll(window, back, 0)[8:] * taps[3 - back : 4 - back, lanes]
            conv = total.astype(jnp.bfloat16)
            both = jnp.dot(conv, maps[g], preferred_element_type=jnp.float32)
            at = aligned(i * chunk, chunk, 8)
            log_decay = sigmoid(both[:, :LANES]) * coef[:, lanes] + a_s[g, at, :]
            decay = jnp.exp(log_decay)
            loss = -jnp.tanh(log_decay) * (decay * decay + 1.0)
            drive = jnp.sqrt(loss) * sigmoid(both[:, LANES:]) * conv.astype(jnp.float32)
            a_s[g, at, :] = decay
            b_s[g, at, :] = drive

    pl.loop(1, length // chunk)(gates)
    gate_load.wait()
    chunk2 = 176

    def gate_values(i):
        at = aligned(i * chunk2, chunk2, 16)
        for g in range(groups):
            gel[g, at, :] = gelu(gateb[at, g * LANES : (g + 1) * LANES].astype(jnp.float32))

    pl.semaphore_wait(barrier, len(partners))

    halo_copy = pltpu.make_async_remote_copy(
        src_ref=mix_hbm.at[pl.ds(length - 16, 16), :],
        dst_ref=halo,
        send_sem=halo_sem.at[0],
        recv_sem=halo_sem.at[1],
        device_id=sp_id(after),
        device_id_type=pl.DeviceIdType.MESH,
    )
    halo_copy.start()
    for copy in loads:
        copy.wait()
    ring_start(0, 0)
    pl.loop(0, length // chunk2)(gate_values)
    halo_copy.wait_recv()
    edge = halo[...].astype(jnp.float32)[8:, :]
    xpad[pl.ds(0, 8), :] = jnp.where(sp > 0, edge, 0.0)
    gates(0)

    stretch = length // SEGMENTS

    def scan_step(i, carry):
        result = []
        for g in range(groups):
            product, state = carry[g]
            at = pl.ds(i, SEGMENTS, stride=stretch)
            decay = a_s[g, at, :]
            state = decay * state + b_s[g, at, :]
            product = product * decay
            a_s[g, at, :] = product
            b_s[g, at, :] = state
            result.append((product, state))
        return tuple(result)

    unit = jnp.ones((SEGMENTS, LANES), jnp.float32)
    ends = lax.fori_loop(0, stretch, scan_step, tuple((unit, unit * 0.0) for _ in range(groups)), unroll=4)
    segments = []
    for g in range(groups):
        product, state = ends[g]
        passed, held = unit[:1], unit[:1] * 0.0
        firsts, seconds = [], []
        for s in range(SEGMENTS):
            firsts.append(passed)
            seconds.append(held)
            held = product[s : s + 1] * held + state[s : s + 1]
            passed = passed * product[s : s + 1]
        segments.append((jnp.concatenate(firsts, axis=0), jnp.concatenate(seconds, axis=0)))
        own_ab[0:1, pl.ds(g * LANES, LANES)] = passed
        own_ab[1:2, pl.ds(g * LANES, LANES)] = held

    def team_copy(k):
        return pltpu.make_async_remote_copy(
            src_ref=own_ab,
            dst_ref=team_ab.at[TEAM - 1 - k],
            send_sem=team_send.at[k - 1],
            recv_sem=team_recv.at[k - 1],
            device_id=sp_id(mate(k)),
            device_id_type=pl.DeviceIdType.MESH,
        )

    def far_copy(k):
        return pltpu.make_async_remote_copy(
            src_ref=team_total,
            dst_ref=far_ab.at[k - 1],
            send_sem=far_send.at[k - 1],
            recv_sem=far_recv.at[k - 1],
            device_id=sp_id(far_mate(k)),
            device_id_type=pl.DeviceIdType.MESH,
        )

    for k in range(1, TEAM):
        team_copy(k).start()
    ring_start(0, 1)
    twin_copy(wgv.at[own_rows, :], 0).start()

    for k in range(1, TEAM):
        team_copy(k).wait_recv()
    own = own_ab[...]
    head_a, head_b = jnp.ones_like(own[0:1]), jnp.zeros_like(own[0:1])
    tail_a, tail_b = own[0:1], own[1:2]
    for k in range(TEAM - 1, 0, -1):
        pair = team_ab[TEAM - 1 - k]
        inside = k <= place
        head_b = jnp.where(inside, pair[0:1] * head_b + pair[1:2], head_b)
        head_a = jnp.where(inside, pair[0:1] * head_a, head_a)
    for k in range(TEAM - 1, 0, -1):
        pair = team_ab[TEAM - 1 - k]
        behind = k > place
        tail_b = jnp.where(behind, pair[0:1] * tail_b + pair[1:2], tail_b)
        tail_a = jnp.where(behind, pair[0:1] * tail_a, tail_a)
    team_total[0:1, :] = head_a * tail_a
    team_total[1:2, :] = tail_a * head_b + tail_b
    for k in range(1, teams):
        far_copy(k).start()
    reached[...] = jnp.zeros_like(reached)
    for k in range(teams - 1, 0, -1):

        @pl.when(k <= team)
        def _():
            far_copy(k).wait_recv()
            pair = far_ab[k - 1]
            reached[...] = pair[0:1] * reached[...] + pair[1:2]

    carried = head_a * reached[...] + head_b

    inflow = [
        segments[g][0] * carried[:, g * LANES : (g + 1) * LANES] + segments[g][1]
        for g in range(groups)
    ]

    def finish_step(i):
        for g in range(groups):
            at = pl.ds(i, SEGMENTS, stride=stretch)
            state = a_s[g, at, :] * inflow[g] + b_s[g, at, :]
            b_s[g, at, :] = state * gel[g, at, :]

    pl.loop(0, stretch, unroll=8)(finish_step)
    for g in range(groups):
        branch[:, pl.ds(g * LANES, LANES)] = b_s[g].astype(jnp.bfloat16)
    outw_load.wait()

    def reduce_scatter(partial, send, recv, ssem, rsem, finish, pumps):
        copies = []
        for s in range(num_tp):
            for q in range(2):
                for way in range(2):
                    shift = num_tp - 1 - s if way == 0 else 1 + s
                    block = lax.rem(t + shift, num_tp)
                    column = way * half + q * sub
                    value = partial(block, column)
                    if s > 0:
                        copies[4 * (s - 1) + 2 * q + way].wait_recv()
                        value = value + recv[way, s - 1, q].astype(jnp.float32)
                    if s < num_tp - 1:
                        send[way, s, q] = value.astype(jnp.bfloat16)
                        copy = pltpu.make_async_remote_copy(
                            src_ref=send.at[way, s, q],
                            dst_ref=recv.at[way, s, q],
                            send_sem=ssem.at[way, s, q],
                            recv_sem=rsem.at[way, s, q],
                            device_id=tp_id(t_next[way]),
                            device_id_type=pl.DeviceIdType.MESH,
                        )
                        copy.start()
                        copies.append(copy)
                    else:
                        finish(column, value)
                pump(pumps[2 * s + q])
        return copies

    def mix_partial(block, column):
        return jnp.dot(
            branch[aligned(block * rows, rows, 16), :],
            outw[:, pl.ds(column, sub)],
            preferred_element_type=jnp.float32,
        )

    def keep_mixed(column, value):
        mixed[:, pl.ds(column, sub)] = value.astype(jnp.bfloat16)

    rs1_copies = reduce_scatter(
        mix_partial, rs1_send, rs1_recv, rs1_ssem, rs1_rsem, keep_mixed, (2, 1, 2, 1, 2, 1, 2, 1)
    )
    resid_load.wait()

    def scaled(value, gain):
        mean = jnp.mean(value * value, axis=-1, keepdims=True)
        return value * lax.rsqrt(mean + EPS) * gain[...]

    def norm_rows(i):
        at = aligned(i * 16, 16, 16)
        stream = resid[at, :].astype(jnp.float32)
        stream += scaled(mixed[at, :].astype(jnp.float32), mix_gain)
        stream = stream.astype(jnp.bfloat16)
        hidden[at, :] = stream
        normed[aligned(t * rows + i * 16, 16, 16), :] = scaled(
            stream.astype(jnp.float32), inner_gain
        ).astype(jnp.bfloat16)

    cut = (rows // 32 + 1) * 16
    parts = ((0, cut), (cut, rows - cut))
    order = tuple(
        tuple((part, side) for part in range(2) for side in (way, 1 - way))
        + tuple((part, way) for part in range(2))
        for way in range(2)
    )

    def gather_ref(way, index, hops):
        part, side = order[way][index]
        block = lax.rem(t + (num_tp - hops if way == 0 else hops), num_tp)
        first, size = parts[part]
        return normed.at[aligned(block * rows + first, size, 16), pl.ds(side * half, half)]

    def gather_copy(way, index):
        ref = gather_ref(way, index, 0 if index < 4 else 1)
        return remote(ref, ag_ssem.at[way, index], ag_rsem.at[way, index], tp_id(t_next[way]))

    def gather_wait(way, index):
        ref = gather_ref(way, index, 1 if index < 4 else 2)
        remote(
            ref, ag_ssem.at[way, index], ag_rsem.at[way, index], tp_id(t_next[way])
        ).wait_recv()

    for part in range(2):
        first, size = parts[part]
        pl.loop(first // 16, (first + size) // 16, unroll=size // 16)(norm_rows)
        for index in range(2 * part, 2 * part + 2):
            for way in range(2):
                gather_copy(way, index).start()
    pump(3)
    for way in range(2):
        gather_wait(way, 0)
        gather_copy(way, 4).start()
    pump(3)
    for way in range(2):
        gather_wait(way, 1)
        gather_wait(way, 2)
        gather_copy(way, 5).start()

    tail_copy = pltpu.make_async_remote_copy(
        src_ref=up.at[pl.ds(length, 16), :],
        dst_ref=up.at[pl.ds(0, 16), :],
        send_sem=tail_sem.at[0],
        recv_sem=tail_sem.at[1],
        device_id=sp_id(after),
        device_id_type=pl.DeviceIdType.MESH,
    )

    def up_block(block):
        source = aligned(block * rows, rows, 16)
        target = aligned(16 + block * rows, rows, 16)

        def tile(j):
            columns = aligned(j * 2 * LANES, 2 * LANES, LANES)
            up[target, columns] = jnp.dot(
                normed[source, :], wgv[:, columns], preferred_element_type=jnp.float32
            ).astype(jnp.bfloat16)

        pl.loop(0, tiles, unroll=tiles)(tile)

        @pl.when(block == num_tp - 1)
        def _():
            tail_copy.start()

    def act_block(block):
        @pl.when(block == 0)
        def _():
            tail_copy.wait_recv()

            @pl.when(sp == 0)
            def _():
                up[pl.ds(0, 16), :] = jnp.zeros((16, 2 * width), jnp.bfloat16)

        window = aligned(block * rows, rows + 16, 16)
        target = aligned(block * rows, rows, 16)

        def tile(j):
            columns = aligned(j * LANES, LANES, LANES)
            results = []
            for side, kernel in enumerate((gate_kernel, value_kernel)):
                start = (2 * j + side) * LANES
                value = up[window, aligned(start, LANES, LANES)].astype(jnp.float32)
                tap = kernel[:, columns].astype(jnp.float32)
                total = value[16:] * tap[2:3]
                for back in range(1, 3):
                    total += pltpu.roll(value, back, 0)[16:] * tap[2 - back : 3 - back]
                results.append(total)
            act[target, columns] = (gelu(results[0]) * results[1]).astype(jnp.bfloat16)

        pl.loop(0, tiles)(tile)

    def around(k):
        return lax.rem(t + k, num_tp)

    pump(first_done - progress[0])
    rival = wgv.at[pl.ds(0, chips * shard), :]
    pltpu.make_async_copy(rival, rival, twin_recv.at[0]).wait()
    up_block(around(0))
    pump(2)
    gather_wait(0, 3)
    up_block(around(num_tp - 1))
    pump(2)
    gather_wait(1, 3)
    up_block(around(1))
    pump(2)
    act_block(around(0))
    act_block(around(1))
    pump(1)
    for index in range(4, 6):
        for way in range(2):
            gather_wait(way, index)
    up_block(around(2))
    act_block(around(num_tp - 1))
    act_block(around(2))
    pump(len(events))
    rival = wd.at[pl.ds(0, chips * shard), :]
    pltpu.make_async_copy(rival, rival, twin_recv.at[1]).wait()

    def down_partial(block, column):
        return lax.dot_general(
            act[aligned(block * rows, rows, 16), :],
            wd[pl.ds(column, sub), :],
            (((1,), (1,)), ((), ())),
            preferred_element_type=jnp.float32,
        )

    rs2_copies = reduce_scatter(
        down_partial, rs2_send, rs2_recv, rs2_ssem, rs2_rsem, keep_mixed, (0,) * 8
    )

    def last_rows(i):
        at = aligned(i * 16, 16, 16)
        stream = hidden[at, :].astype(jnp.float32)
        stream += scaled(mixed[at, :].astype(jnp.float32), final_gain)
        out_ref[at, :] = stream.astype(jnp.bfloat16)

    pl.loop(0, rows // 16, unroll=rows // 16)(last_rows)

    halo_copy.wait_send()
    tail_copy.wait_send()
    for k in range(1, TEAM):
        team_copy(k).wait_send()
    for k in range(1, teams):
        far_copy(k).wait_send()

        @pl.when(k > team)
        def _():
            far_copy(k).wait_recv()

    for stage in range(2):
        for way in range(2):
            for index in range(per_stage):
                ring_copy(way, stage, index).wait_send()
            for distance in range(1, far + 1 - way):
                pair_copy(way, stage, distance).wait_send()
    gathered = wgv.at[pl.ds(0, chips * shard), :]
    pltpu.make_async_copy(gathered, gathered, twin_send.at[0]).wait()
    gathered = wd.at[pl.ds(0, chips * shard), :]
    pltpu.make_async_copy(gathered, gathered, twin_send.at[1]).wait()
    for copy in rs1_copies + rs2_copies:
        copy.wait_send()
    for index in range(6):
        for way in range(2):
            gather_copy(way, index).wait_send()


def local(
    num_sp,
    num_tp,
    residual,
    mix_input,
    gate_input,
    mix_kernel,
    recur_gate_map,
    input_gate_map,
    decay_param,
    jump_log,
    out_weight,
    mix_gain,
    inner_gain,
    final_gain,
    gate_weight,
    value_weight,
    gate_kernel,
    value_kernel,
    down_weight,
):
    length, channels = mix_input.shape
    model = residual.shape[1]
    shard, width = gate_weight.shape
    rows = length // num_tp
    sub = model // 4
    groups = channels // LANES
    far = num_sp // 4
    steps = 2 * (2 * far - 1)
    hbm = pl.BlockSpec(memory_space=pl.ANY)
    vmem = pl.BlockSpec(memory_space=pltpu.VMEM)
    bf16, f32 = jnp.bfloat16, jnp.float32
    dma = pltpu.SemaphoreType.DMA
    flow = (2, num_tp - 1, 2, rows, sub)
    return pl.pallas_call(
        functools.partial(layer_kernel, num_sp, num_tp),
        out_shape=jax.ShapeDtypeStruct((rows, model), bf16),
        in_specs=[hbm] * 8 + [vmem] * 9,
        out_specs=vmem,
        scratch_shapes=[
            pltpu.VMEM((num_sp * shard, 2 * width), bf16),
            pltpu.VMEM((num_sp * shard, width), bf16),
            pltpu.VMEM((length, channels), bf16),
            pltpu.VMEM((16, channels), bf16),
            pltpu.VMEM((length, channels), bf16),
            pltpu.VMEM((groups, length, LANES), f32),
            pltpu.VMEM((groups, length, LANES), f32),
            pltpu.VMEM((groups, length, LANES), f32),
            pltpu.VMEM((length + 8, channels), f32),
            pltpu.VMEM((groups, LANES, 2 * LANES), bf16),
            pltpu.VMEM((length, channels), bf16),
            pltpu.VMEM((channels, model), bf16),
            pltpu.VMEM((rows, model), bf16),
            pltpu.VMEM((2, channels), f32),
            pltpu.VMEM((TEAM - 1, 2, channels), f32),
            pltpu.VMEM((2, channels), f32),
            pltpu.VMEM((num_sp // TEAM - 1, 2, channels), f32),
            pltpu.VMEM((1, channels), f32),
            pltpu.VMEM(flow, bf16),
            pltpu.VMEM(flow, bf16),
            pltpu.VMEM(flow, bf16),
            pltpu.VMEM(flow, bf16),
            pltpu.VMEM((rows, model), bf16),
            pltpu.VMEM((rows, model), bf16),
            pltpu.VMEM((length, model), bf16),
            pltpu.VMEM((16 + length, 2 * width), bf16),
            pltpu.VMEM((length, width), bf16),
            dma((5 + groups,)),
            dma((2 * (width // LANES) + 1,)),
            dma((2,)),
            dma((2,)),
            dma((TEAM - 1,)),
            dma((TEAM - 1,)),
            dma((num_sp // TEAM - 1,)),
            dma((num_sp // TEAM - 1,)),
            dma((2, steps)),
            dma((2, steps)),
            dma((steps,)),
            dma((steps,)),
            dma((2,)),
            dma((2,)),
            dma(flow[:3]),
            dma(flow[:3]),
            dma(flow[:3]),
            dma(flow[:3]),
            dma((2, 6)),
            dma((2, 6)),
        ],
        compiler_params=pltpu.CompilerParams(
            collective_id=0, has_side_effects=True, vmem_limit_bytes=67043328
        ),
    )(
        mix_input,
        gate_input,
        jump_log,
        residual,
        out_weight,
        gate_weight,
        value_weight,
        down_weight.T,
        mix_kernel,
        recur_gate_map,
        input_gate_map,
        decay_param.reshape(1, channels),
        mix_gain.reshape(1, model),
        inner_gain.reshape(1, model),
        final_gain.reshape(1, model),
        gate_kernel,
        value_kernel,
    )


def solution(mesh):
    return jax.shard_map(
        functools.partial(local, mesh.shape["sp"], mesh.shape["tp"]),
        mesh=mesh,
        in_specs=(
            P(("grp", "sp"), None),
            P(("grp", "sp"), "tp"),
            P(("grp", "sp"), "tp"),
            P(None, "tp"),
            P("tp", None, None),
            P("tp", None, None),
            P("tp"),
            P(("grp", "sp"), "tp"),
            P("tp", None),
            P(),
            P(),
            P(),
            P("sp", "tp"),
            P("sp", "tp"),
            P(None, "tp"),
            P(None, "tp"),
            P("tp", "sp"),
        ),
        out_specs=P(("grp", "sp", "tp"), None),
        check_vma=False,
    )
```

```python
import functools

import jax
import jax.numpy as jnp
from jax import lax
from jax.experimental import pallas as pl
from jax.experimental.pallas import tpu as pltpu
from jax.sharding import PartitionSpec as P

EPS = 1e-06
GATE_SCALE = 8.0
LANES = 128
SEGMENTS = 8
TEAM = 8
SQRT_2_PI = 0.7978845608028654


def gelu(v):
    return 0.5 * v * (1.0 + jnp.tanh(SQRT_2_PI * (v + 0.044715 * (v * v * v))))


def sigmoid(v):
    return 1.0 / (1.0 + jnp.exp(-v))


def softplus(v):
    z = jnp.exp(-jnp.abs(v))
    ratio = z / (2.0 + z)
    square = ratio * ratio
    series = jnp.full_like(square, 1.0 / 19.0)
    for power in range(17, 0, -2):
        series = series * square + 1.0 / power
    return jnp.maximum(v, 0.0) + 2.0 * ratio * series


def aligned(start, size, multiple):
    return pl.ds(pl.multiple_of(start, multiple), size)


def layer_kernel(
    num_sp,
    num_tp,
    mix_hbm,
    gate_hbm,
    jump_hbm,
    resid_hbm,
    outw_hbm,
    gw_hbm,
    vw_hbm,
    dw_hbm,
    mix_kernel,
    recur_map,
    input_map,
    decay_param,
    mix_gain,
    inner_gain,
    final_gain,
    gate_kernel,
    value_kernel,
    out_ref,
    wgv,
    wd,
    mixb,
    halo,
    gateb,
    a_s,
    b_s,
    gel,
    xpad,
    maps,
    branch,
    outw,
    resid,
    own_ab,
    team_ab,
    team_total,
    far_ab,
    reached,
    rs1_send,
    rs1_recv,
    rs2_send,
    rs2_recv,
    ahead,
    mixed,
    hidden,
    normed,
    up,
    act,
    load_sem,
    wload_sem,
    halo_sem,
    tail_sem,
    team_send,
    team_recv,
    far_send,
    far_recv,
    ring_send,
    ring_recv,
    pair_send,
    pair_recv,
    twin_send,
    twin_recv,
    rs1_ssem,
    rs1_rsem,
    rs2_ssem,
    rs2_rsem,
    ag_ssem,
    ag_rsem,
):
    sp = lax.axis_index("sp")
    grp = lax.axis_index("grp")
    parity = lax.rem(grp, 2)
    pair_grp = grp + 1 - 2 * parity
    t = lax.axis_index("tp")
    length, channels = mixb.shape
    groups = channels // LANES
    shard = gw_hbm.shape[0]
    width = gw_hbm.shape[1]
    tiles = width // LANES
    model = outw.shape[1]
    rows = length // num_tp
    half = model // 2
    sub = half // 2
    chips = num_sp // 2
    far = chips // 2
    core = lax.rem(sp, 2)
    chip = sp // 2
    twin = sp + 1 - 2 * core
    after = lax.rem(sp + 1, num_sp)
    before = lax.rem(sp + num_sp - 1, num_sp)
    z_next = (lax.rem(sp + 2, num_sp), lax.rem(sp + num_sp - 2, num_sp))
    t_next = (lax.rem(t + 1, num_tp), lax.rem(t + num_tp - 1, num_tp))
    place = lax.rem(sp, TEAM)
    team = sp // TEAM
    teams = num_sp // TEAM

    def sp_id(index):
        return {"sp": index}

    def tp_id(index):
        return {"tp": index}

    def mate(k):
        return team * TEAM + lax.rem(place + k, TEAM)

    def far_mate(k):
        return lax.rem(sp + TEAM * k, num_sp)

    barrier = pltpu.get_barrier_semaphore()
    partners = [sp_id(after), sp_id(before), sp_id(z_next[0]), sp_id(z_next[1])]
    partners += [sp_id(mate(k)) for k in range(1, TEAM)]
    partners += [sp_id(far_mate(k)) for k in range(1, teams)]
    partners += [tp_id(lax.rem(t + k, num_tp)) for k in range(1, num_tp)]
    partners += [{"grp": pair_grp}]
    for partner in partners:
        pl.semaphore_signal(barrier, inc=1, device_id=partner, device_id_type=pl.DeviceIdType.MESH)

    own_rows = aligned(sp * shard, shard, shard)

    def weight_loads():
        copies = []
        for j in range(tiles):
            for side, source in enumerate((gw_hbm, vw_hbm)):
                copies.append(
                    pltpu.make_async_copy(
                        source.at[:, pl.ds(j * LANES, LANES)],
                        wgv.at[own_rows, pl.ds((2 * j + side) * LANES, LANES)],
                        wload_sem.at[2 * j + side],
                    )
                )
        copies.append(pltpu.make_async_copy(dw_hbm, wd.at[own_rows, :], wload_sem.at[2 * tiles]))
        return copies

    mix_load = pltpu.make_async_copy(mix_hbm, mixb, load_sem.at[0])
    jump_loads = [
        pltpu.make_async_copy(
            jump_hbm.at[:, pl.ds(g * LANES, LANES)], a_s.at[g], load_sem.at[5 + g]
        )
        for g in range(groups)
    ]
    gate_load = pltpu.make_async_copy(gate_hbm, gateb, load_sem.at[1])
    outw_load = pltpu.make_async_copy(outw_hbm, outw, load_sem.at[2])
    resid_load = pltpu.make_async_copy(
        resid_hbm.at[aligned(t * rows, rows, 16), :], resid, load_sem.at[3]
    )
    mix_load.start()
    loads = weight_loads()
    for copy in loads:
        copy.start()
    for copy in jump_loads:
        copy.start()
    gate_load.start()
    outw_load.start()
    resid_load.start()
    for g in range(groups):
        maps[g, :, :LANES] = recur_map[g]
        maps[g, :, LANES:] = input_map[g]

    whole = (wgv, wd)
    lone = ((2 * tiles // 3) * LANES, ((tiles + 1) // 3) * LANES)
    near = 2 * (far - 1)
    per_stage = near + 1

    def part_ref(stage, origin, part, side):
        ref, size = whole[stage], lone[stage]
        at = aligned((2 * origin + core) * shard, shard, shard)
        if part == 0:
            return ref.at[at, aligned(side * size, size, LANES)]
        return ref.at[at, pl.ds(2 * size, ref.shape[1] - 2 * size)]

    def origin_at(way, distance):
        return lax.rem(chip + (chips - distance if way == 0 else distance), chips)

    def what(way, index):
        return index // 2 + 1, (way if index == near else index % 2)

    def remote(ref, send_sem, recv_sem, device_id):
        return pltpu.make_async_remote_copy(
            src_ref=ref,
            dst_ref=ref,
            send_sem=send_sem,
            recv_sem=recv_sem,
            device_id=device_id,
            device_id_type=pl.DeviceIdType.MESH,
        )

    def ring_copy(way, stage, index, received=False):
        distance, part = what(way, index)
        ref = part_ref(stage, origin_at(way, distance - (0 if received else 1)), part, parity)
        slot = stage * per_stage + index
        return remote(
            ref, ring_send.at[way, slot], ring_recv.at[way, slot], sp_id(z_next[way])
        )

    def pair_copy(way, stage, distance, received=False):
        side = 1 - parity if received else parity
        ref = part_ref(stage, origin_at(way, distance), 0, side)
        slot = stage * per_stage + way * far + distance - 1
        return remote(ref, pair_send.at[slot], pair_recv.at[slot], {"grp": pair_grp})

    def twin_copy(ref, stage):
        return remote(ref, twin_send.at[stage], twin_recv.at[stage], sp_id(twin))

    def arrived(way, stage, index):
        distance, part = what(way, index)
        ring_copy(way, stage, index, True).wait_recv()
        if distance < far - 1:
            ring_copy(way, stage, index + 2).start()
        elif distance == far - 1 and part == way:
            ring_copy(way, stage, near).start()
        if part == 0:
            pair_copy(way, stage, distance).start()
        twin_copy(part_ref(stage, origin_at(way, distance), part, parity), stage).start()

    def crossed(way, stage, distance):
        pair_copy(way, stage, distance, True).wait_recv()
        twin_copy(part_ref(stage, origin_at(way, distance), 0, 1 - parity), stage).start()

    def ring_start(stage, part):
        for way in range(2):
            ring_copy(way, stage, part).start()

    def event(stage, index):
        if index < per_stage:
            for way in range(2):
                arrived(way, stage, index)
            if index % 2 == 1 and index > 1:
                for way in range(2):
                    crossed(way, stage, (index - 1) // 2)
        else:
            for way in range(2):
                crossed(way, stage, far - 1)
            crossed(0, stage, far)

    def at_distance(stage, distance):
        first = 2 * (distance - 1)
        return [(stage, k) for k in range(first, min(first + 2, per_stage))]

    lag = far - 3
    events = []
    for distance in range(1, far + 1):
        events += at_distance(0, distance)
        if distance > lag:
            events += at_distance(1, distance - lag)
        if distance == lag:
            down_start = len(events)
    events.append((0, per_stage))
    first_done = len(events)
    for distance in range(far - lag + 1, far + 1):
        events += at_distance(1, distance)
    events.append((1, per_stage))
    progress = [0]

    def pump(count):
        for _ in range(count):
            number = progress[0]
            if number >= len(events):
                return
            if number == down_start:
                ring_start(1, 0)
                ring_start(1, 1)
                twin_copy(wd.at[own_rows, :], 1).start()
            event(*events[number])
            progress[0] = number + 1

    mix_load.wait()
    for g in range(groups):
        jump_loads[g].wait()
    xpad[pl.ds(8, length), :] = mixb[...].astype(jnp.float32)
    taps = mix_kernel[...].astype(jnp.float32)
    coef = -GATE_SCALE * softplus(-decay_param[...])
    chunk = 64

    def gates(i):
        for g in range(groups):
            lanes = slice(g * LANES, (g + 1) * LANES)
            window = xpad[aligned(i * chunk, chunk + 8, 8), lanes]
            total = window[8:] * taps[3:4, lanes]
            for back in range(1, 4):
                total += pltpu.roll(window, back, 0)[8:] * taps[3 - back : 4 - back, lanes]
            conv = total.astype(jnp.bfloat16)
            both = jnp.dot(conv, maps[g], preferred_element_type=jnp.float32)
            at = aligned(i * chunk, chunk, 8)
            log_decay = sigmoid(both[:, :LANES]) * coef[:, lanes] + a_s[g, at, :]
            decay = jnp.exp(log_decay)
            loss = -jnp.tanh(log_decay) * (decay * decay + 1.0)
            drive = jnp.sqrt(loss) * sigmoid(both[:, LANES:]) * conv.astype(jnp.float32)
            a_s[g, at, :] = decay
            b_s[g, at, :] = drive

    pl.loop(1, length // chunk)(gates)
    gate_load.wait()
    chunk2 = 176

    def gate_values(i):
        at = aligned(i * chunk2, chunk2, 16)
        for g in range(groups):
            gel[g, at, :] = gelu(gateb[at, g * LANES : (g + 1) * LANES].astype(jnp.float32))

    pl.semaphore_wait(barrier, len(partners))

    halo_copy = pltpu.make_async_remote_copy(
        src_ref=mix_hbm.at[pl.ds(length - 16, 16), :],
        dst_ref=halo,
        send_sem=halo_sem.at[0],
        recv_sem=halo_sem.at[1],
        device_id=sp_id(after),
        device_id_type=pl.DeviceIdType.MESH,
    )
    halo_copy.start()
    for copy in loads:
        copy.wait()
    ring_start(0, 0)
    pl.loop(0, length // chunk2)(gate_values)
    halo_copy.wait_recv()
    edge = halo[...].astype(jnp.float32)[8:, :]
    xpad[pl.ds(0, 8), :] = jnp.where(sp > 0, edge, 0.0)
    gates(0)

    stretch = length // SEGMENTS

    def scan_step(i, carry):
        result = []
        for g in range(groups):
            product, state = carry[g]
            at = pl.ds(i, SEGMENTS, stride=stretch)
            decay = a_s[g, at, :]
            state = decay * state + b_s[g, at, :]
            product = product * decay
            a_s[g, at, :] = product
            b_s[g, at, :] = state
            result.append((product, state))
        return tuple(result)

    unit = jnp.ones((SEGMENTS, LANES), jnp.float32)
    ends = lax.fori_loop(0, stretch, scan_step, tuple((unit, unit * 0.0) for _ in range(groups)), unroll=4)
    segments = []
    for g in range(groups):
        product, state = ends[g]
        passed, held = unit[:1], unit[:1] * 0.0
        firsts, seconds = [], []
        for s in range(SEGMENTS):
            firsts.append(passed)
            seconds.append(held)
            held = product[s : s + 1] * held + state[s : s + 1]
            passed = passed * product[s : s + 1]
        segments.append((jnp.concatenate(firsts, axis=0), jnp.concatenate(seconds, axis=0)))
        own_ab[0:1, pl.ds(g * LANES, LANES)] = passed
        own_ab[1:2, pl.ds(g * LANES, LANES)] = held

    def team_copy(k):
        return pltpu.make_async_remote_copy(
            src_ref=own_ab,
            dst_ref=team_ab.at[TEAM - 1 - k],
            send_sem=team_send.at[k - 1],
            recv_sem=team_recv.at[k - 1],
            device_id=sp_id(mate(k)),
            device_id_type=pl.DeviceIdType.MESH,
        )

    def far_copy(k):
        return pltpu.make_async_remote_copy(
            src_ref=team_total,
            dst_ref=far_ab.at[k - 1],
            send_sem=far_send.at[k - 1],
            recv_sem=far_recv.at[k - 1],
            device_id=sp_id(far_mate(k)),
            device_id_type=pl.DeviceIdType.MESH,
        )

    for k in range(1, TEAM):
        team_copy(k).start()
    ring_start(0, 1)
    twin_copy(wgv.at[own_rows, :], 0).start()
    pump(1)

    for k in range(1, TEAM):
        team_copy(k).wait_recv()
    own = own_ab[...]
    head_a, head_b = jnp.ones_like(own[0:1]), jnp.zeros_like(own[0:1])
    tail_a, tail_b = own[0:1], own[1:2]
    for k in range(TEAM - 1, 0, -1):
        pair = team_ab[TEAM - 1 - k]
        inside = k <= place
        head_b = jnp.where(inside, pair[0:1] * head_b + pair[1:2], head_b)
        head_a = jnp.where(inside, pair[0:1] * head_a, head_a)
    for k in range(TEAM - 1, 0, -1):
        pair = team_ab[TEAM - 1 - k]
        behind = k > place
        tail_b = jnp.where(behind, pair[0:1] * tail_b + pair[1:2], tail_b)
        tail_a = jnp.where(behind, pair[0:1] * tail_a, tail_a)
    team_total[0:1, :] = head_a * tail_a
    team_total[1:2, :] = tail_a * head_b + tail_b
    for k in range(1, teams):
        far_copy(k).start()
    pump(2)
    reached[...] = jnp.zeros_like(reached)
    for k in range(teams - 1, 0, -1):

        @pl.when(k <= team)
        def _():
            far_copy(k).wait_recv()
            pair = far_ab[k - 1]
            reached[...] = pair[0:1] * reached[...] + pair[1:2]

    carried = head_a * reached[...] + head_b
    pump(1)

    inflow = [
        segments[g][0] * carried[:, g * LANES : (g + 1) * LANES] + segments[g][1]
        for g in range(groups)
    ]

    def finish_step(i):
        for g in range(groups):
            at = pl.ds(i, SEGMENTS, stride=stretch)
            state = a_s[g, at, :] * inflow[g] + b_s[g, at, :]
            b_s[g, at, :] = state * gel[g, at, :]

    pl.loop(0, stretch, unroll=8)(finish_step)
    for g in range(groups):
        branch[:, pl.ds(g * LANES, LANES)] = b_s[g].astype(jnp.bfloat16)
    outw_load.wait()

    def reduce_scatter(partial, send, recv, ssem, rsem, finish, pumps):
        copies = {}

        def term(s, q, way):
            shift = num_tp - 1 - s if way == 0 else 1 + s
            return partial(lax.rem(t + shift, num_tp), way * half + q * sub)

        for s in range(num_tp):
            for q in range(2):
                for way in range(2):
                    if s == 0:
                        value = term(s, q, way)
                    else:
                        copies[s - 1, q, way].wait_recv()
                        value = ahead[way, q] + recv[way, s - 1, q].astype(jnp.float32)
                    if s < num_tp - 1:
                        send[way, s, q] = value.astype(jnp.bfloat16)
                        copy = pltpu.make_async_remote_copy(
                            src_ref=send.at[way, s, q],
                            dst_ref=recv.at[way, s, q],
                            send_sem=ssem.at[way, s, q],
                            recv_sem=rsem.at[way, s, q],
                            device_id=tp_id(t_next[way]),
                            device_id_type=pl.DeviceIdType.MESH,
                        )
                        copy.start()
                        copies[s, q, way] = copy
                    else:
                        finish(way * half + q * sub, value)
                if s < num_tp - 1:
                    for way in range(2):
                        ahead[way, q] = term(s + 1, q, way)
                pump(pumps[2 * s + q])
        return list(copies.values())

    def mix_partial(block, column):
        return jnp.dot(
            branch[aligned(block * rows, rows, 16), :],
            outw[:, pl.ds(column, sub)],
            preferred_element_type=jnp.float32,
        )

    def keep_mixed(column, value):
        mixed[:, pl.ds(column, sub)] = value.astype(jnp.bfloat16)

    rs1_copies = reduce_scatter(
        mix_partial, rs1_send, rs1_recv, rs1_ssem, rs1_rsem, keep_mixed, (1, 2, 1, 2, 1, 2, 1, 1)
    )
    resid_load.wait()

    def scaled(value, gain):
        mean = jnp.mean(value * value, axis=-1, keepdims=True)
        return value * lax.rsqrt(mean + EPS) * gain[...]

    def norm_rows(i):
        at = aligned(i * 16, 16, 16)
        stream = resid[at, :].astype(jnp.float32)
        stream += scaled(mixed[at, :].astype(jnp.float32), mix_gain)
        stream = stream.astype(jnp.bfloat16)
        hidden[at, :] = stream
        normed[aligned(t * rows + i * 16, 16, 16), :] = scaled(
            stream.astype(jnp.float32), inner_gain
        ).astype(jnp.bfloat16)

    cut = (rows // 32 + 1) * 16
    parts = ((0, cut), (cut, rows - cut))
    order = tuple(
        tuple((part, side) for part in range(2) for side in (way, 1 - way))
        + tuple((part, way) for part in range(2))
        for way in range(2)
    )

    def gather_ref(way, index, hops):
        part, side = order[way][index]
        block = lax.rem(t + (num_tp - hops if way == 0 else hops), num_tp)
        first, size = parts[part]
        return normed.at[aligned(block * rows + first, size, 16), pl.ds(side * half, half)]

    def gather_copy(way, index):
        ref = gather_ref(way, index, 0 if index < 4 else 1)
        return remote(ref, ag_ssem.at[way, index], ag_rsem.at[way, index], tp_id(t_next[way]))

    def gather_wait(way, index):
        ref = gather_ref(way, index, 1 if index < 4 else 2)
        remote(
            ref, ag_ssem.at[way, index], ag_rsem.at[way, index], tp_id(t_next[way])
        ).wait_recv()

    for part in range(2):
        first, size = parts[part]
        pl.loop(first // 16, (first + size) // 16, unroll=size // 16)(norm_rows)
        for index in range(2 * part, 2 * part + 2):
            for way in range(2):
                gather_copy(way, index).start()
    pump(4)
    for way in range(2):
        gather_wait(way, 0)
        gather_copy(way, 4).start()
    pump(3)
    for way in range(2):
        gather_wait(way, 1)
        gather_wait(way, 2)
        gather_copy(way, 5).start()

    tail_copy = pltpu.make_async_remote_copy(
        src_ref=up.at[pl.ds(length, 16), :],
        dst_ref=up.at[pl.ds(0, 16), :],
        send_sem=tail_sem.at[0],
        recv_sem=tail_sem.at[1],
        device_id=sp_id(after),
        device_id_type=pl.DeviceIdType.MESH,
    )

    def act_ready(block):
        @pl.when(block == 0)
        def _():
            tail_copy.wait_recv()

            @pl.when(sp == 0)
            def _():
                up[pl.ds(0, 16), :] = jnp.zeros((16, 2 * width), jnp.bfloat16)

    def act_tile(block, j):
        columns = aligned(j * LANES, LANES, LANES)
        results = []
        for side, kernel in enumerate((gate_kernel, value_kernel)):
            start = (2 * j + side) * LANES
            value = up[
                aligned(block * rows, rows + 16, 16), aligned(start, LANES, LANES)
            ].astype(jnp.float32)
            tap = kernel[:, columns].astype(jnp.float32)
            total = value[16:] * tap[2:3]
            for back in range(1, 3):
                total += pltpu.roll(value, back, 0)[16:] * tap[2 - back : 3 - back]
            results.append(total)
        act[aligned(block * rows, rows, 16), columns] = (gelu(results[0]) * results[1]).astype(
            jnp.bfloat16
        )

    def act_block(block):
        act_ready(block)
        pl.loop(0, tiles)(lambda j: act_tile(block, j))

    def up_block(block, beside=None):
        if beside is not None:
            act_ready(beside)

        def tile(j):
            columns = aligned(j * 2 * LANES, 2 * LANES, LANES)
            if beside is not None:
                act_tile(beside, j)
            up[aligned(16 + block * rows, rows, 16), columns] = jnp.dot(
                normed[aligned(block * rows, rows, 16), :],
                wgv[:, columns],
                preferred_element_type=jnp.float32,
            ).astype(jnp.bfloat16)

        pl.loop(0, tiles, unroll=tiles)(tile)

        @pl.when(block == num_tp - 1)
        def _():
            tail_copy.start()

    def around(k):
        return lax.rem(t + k, num_tp)

    pump(first_done - progress[0])
    rival = wgv.at[pl.ds(0, chips * shard), :]
    pltpu.make_async_copy(rival, rival, twin_recv.at[0]).wait()
    up_block(around(0))
    pump(2)
    gather_wait(0, 3)
    up_block(around(num_tp - 1))
    pump(2)
    gather_wait(1, 3)
    up_block(around(1))
    pump(2)
    act_block(around(0))
    pump(2)
    for index in range(4, 6):
        for way in range(2):
            gather_wait(way, index)
    up_block(around(2), around(1))
    pump(1)
    act_block(around(num_tp - 1))
    act_block(around(2))
    pump(len(events))
    rival = wd.at[pl.ds(0, chips * shard), :]
    pltpu.make_async_copy(rival, rival, twin_recv.at[1]).wait()

    def down_partial(block, column):
        return lax.dot_general(
            act[aligned(block * rows, rows, 16), :],
            wd[pl.ds(column, sub), :],
            (((1,), (1,)), ((), ())),
            preferred_element_type=jnp.float32,
        )

    rs2_copies = reduce_scatter(
        down_partial, rs2_send, rs2_recv, rs2_ssem, rs2_rsem, keep_mixed, (0,) * 8
    )

    def last_rows(i):
        at = aligned(i * 16, 16, 16)
        stream = hidden[at, :].astype(jnp.float32)
        stream += scaled(mixed[at, :].astype(jnp.float32), final_gain)
        out_ref[at, :] = stream.astype(jnp.bfloat16)

    pl.loop(0, rows // 16, unroll=rows // 16)(last_rows)

    halo_copy.wait_send()
    tail_copy.wait_send()
    for k in range(1, TEAM):
        team_copy(k).wait_send()
    for k in range(1, teams):
        far_copy(k).wait_send()

        @pl.when(k > team)
        def _():
            far_copy(k).wait_recv()

    for stage in range(2):
        for way in range(2):
            for index in range(per_stage):
                ring_copy(way, stage, index).wait_send()
            for distance in range(1, far + 1 - way):
                pair_copy(way, stage, distance).wait_send()
    gathered = wgv.at[pl.ds(0, chips * shard), :]
    pltpu.make_async_copy(gathered, gathered, twin_send.at[0]).wait()
    gathered = wd.at[pl.ds(0, chips * shard), :]
    pltpu.make_async_copy(gathered, gathered, twin_send.at[1]).wait()
    for copy in rs1_copies + rs2_copies:
        copy.wait_send()
    for index in range(6):
        for way in range(2):
            gather_copy(way, index).wait_send()


def local(
    num_sp,
    num_tp,
    residual,
    mix_input,
    gate_input,
    mix_kernel,
    recur_gate_map,
    input_gate_map,
    decay_param,
    jump_log,
    out_weight,
    mix_gain,
    inner_gain,
    final_gain,
    gate_weight,
    value_weight,
    gate_kernel,
    value_kernel,
    down_weight,
):
    length, channels = mix_input.shape
    model = residual.shape[1]
    shard, width = gate_weight.shape
    rows = length // num_tp
    sub = model // 4
    groups = channels // LANES
    far = num_sp // 4
    steps = 2 * (2 * far - 1)
    hbm = pl.BlockSpec(memory_space=pl.ANY)
    vmem = pl.BlockSpec(memory_space=pltpu.VMEM)
    bf16, f32 = jnp.bfloat16, jnp.float32
    dma = pltpu.SemaphoreType.DMA
    flow = (2, num_tp - 1, 2, rows, sub)
    return pl.pallas_call(
        functools.partial(layer_kernel, num_sp, num_tp),
        out_shape=jax.ShapeDtypeStruct((rows, model), bf16),
        in_specs=[hbm] * 8 + [vmem] * 9,
        out_specs=vmem,
        scratch_shapes=[
            pltpu.VMEM((num_sp * shard, 2 * width), bf16),
            pltpu.VMEM((num_sp * shard, width), bf16),
            pltpu.VMEM((length, channels), bf16),
            pltpu.VMEM((16, channels), bf16),
            pltpu.VMEM((length, channels), bf16),
            pltpu.VMEM((groups, length, LANES), f32),
            pltpu.VMEM((groups, length, LANES), f32),
            pltpu.VMEM((groups, length, LANES), f32),
            pltpu.VMEM((length + 8, channels), f32),
            pltpu.VMEM((groups, LANES, 2 * LANES), bf16),
            pltpu.VMEM((length, channels), bf16),
            pltpu.VMEM((channels, model), bf16),
            pltpu.VMEM((rows, model), bf16),
            pltpu.VMEM((2, channels), f32),
            pltpu.VMEM((TEAM - 1, 2, channels), f32),
            pltpu.VMEM((2, channels), f32),
            pltpu.VMEM((num_sp // TEAM - 1, 2, channels), f32),
            pltpu.VMEM((1, channels), f32),
            pltpu.VMEM(flow, bf16),
            pltpu.VMEM(flow, bf16),
            pltpu.VMEM(flow, bf16),
            pltpu.VMEM(flow, bf16),
            pltpu.VMEM((2, 2, rows, sub), f32),
            pltpu.VMEM((rows, model), bf16),
            pltpu.VMEM((rows, model), bf16),
            pltpu.VMEM((length, model), bf16),
            pltpu.VMEM((16 + length, 2 * width), bf16),
            pltpu.VMEM((length, width), bf16),
            dma((5 + groups,)),
            dma((2 * (width // LANES) + 1,)),
            dma((2,)),
            dma((2,)),
            dma((TEAM - 1,)),
            dma((TEAM - 1,)),
            dma((num_sp // TEAM - 1,)),
            dma((num_sp // TEAM - 1,)),
            dma((2, steps)),
            dma((2, steps)),
            dma((steps,)),
            dma((steps,)),
            dma((2,)),
            dma((2,)),
            dma(flow[:3]),
            dma(flow[:3]),
            dma(flow[:3]),
            dma(flow[:3]),
            dma((2, 6)),
            dma((2, 6)),
        ],
        compiler_params=pltpu.CompilerParams(
            collective_id=0, has_side_effects=True, vmem_limit_bytes=67043328
        ),
    )(
        mix_input,
        gate_input,
        jump_log,
        residual,
        out_weight,
        gate_weight,
        value_weight,
        down_weight.T,
        mix_kernel,
        recur_gate_map,
        input_gate_map,
        decay_param.reshape(1, channels),
        mix_gain.reshape(1, model),
        inner_gain.reshape(1, model),
        final_gain.reshape(1, model),
        gate_kernel,
        value_kernel,
    )


def solution(mesh):
    return jax.shard_map(
        functools.partial(local, mesh.shape["sp"], mesh.shape["tp"]),
        mesh=mesh,
        in_specs=(
            P(("grp", "sp"), None),
            P(("grp", "sp"), "tp"),
            P(("grp", "sp"), "tp"),
            P(None, "tp"),
            P("tp", None, None),
            P("tp", None, None),
            P("tp"),
            P(("grp", "sp"), "tp"),
            P("tp", None),
            P(),
            P(),
            P(),
            P("sp", "tp"),
            P("sp", "tp"),
            P(None, "tp"),
            P(None, "tp"),
            P("tp", "sp"),
        ),
        out_specs=P(("grp", "sp", "tp"), None),
        check_vma=False,
    )
```

```python
import functools

import jax
import jax.numpy as jnp
from jax import lax
from jax.experimental import pallas as pl
from jax.experimental.pallas import tpu as pltpu
from jax.sharding import PartitionSpec as P

EPS = 1e-06
GATE_SCALE = 8.0
LANES = 128
SEGMENTS = 8
TEAM = 8
SQRT_2_PI = 0.7978845608028654


def gelu(v):
    return 0.5 * v * (1.0 + jnp.tanh(SQRT_2_PI * (v + 0.044715 * (v * v * v))))


def sigmoid(v):
    return 1.0 / (1.0 + jnp.exp(-v))


def softplus(v):
    z = jnp.exp(-jnp.abs(v))
    ratio = z / (2.0 + z)
    square = ratio * ratio
    series = jnp.full_like(square, 1.0 / 19.0)
    for power in range(17, 0, -2):
        series = series * square + 1.0 / power
    return jnp.maximum(v, 0.0) + 2.0 * ratio * series


def aligned(start, size, multiple):
    return pl.ds(pl.multiple_of(start, multiple), size)


def layer_kernel(
    num_sp,
    num_tp,
    mix_hbm,
    gate_hbm,
    jump_hbm,
    resid_hbm,
    outw_hbm,
    gw_hbm,
    vw_hbm,
    dw_hbm,
    mix_kernel,
    recur_map,
    input_map,
    decay_param,
    mix_gain,
    inner_gain,
    final_gain,
    gate_kernel,
    value_kernel,
    out_ref,
    wgv,
    wd,
    mixb,
    halo,
    gateb,
    a_s,
    b_s,
    gel,
    xpad,
    maps,
    branch,
    outw,
    resid,
    own_ab,
    team_ab,
    team_total,
    far_ab,
    reached,
    rs1_send,
    rs1_recv,
    rs2_send,
    rs2_recv,
    ahead,
    mixed,
    hidden,
    normed,
    up,
    act,
    load_sem,
    wload_sem,
    halo_sem,
    tail_sem,
    team_send,
    team_recv,
    far_send,
    far_recv,
    ring_send,
    ring_recv,
    pair_send,
    pair_recv,
    twin_send,
    twin_recv,
    rs1_ssem,
    rs1_rsem,
    rs2_ssem,
    rs2_rsem,
    ag_ssem,
    ag_rsem,
):
    sp = lax.axis_index("sp")
    grp = lax.axis_index("grp")
    parity = lax.rem(grp, 2)
    pair_grp = grp + 1 - 2 * parity
    t = lax.axis_index("tp")
    length, channels = mixb.shape
    groups = channels // LANES
    shard = gw_hbm.shape[0]
    width = gw_hbm.shape[1]
    tiles = width // LANES
    model = outw.shape[1]
    rows = length // num_tp
    half = model // 2
    sub = half // 2
    chips = num_sp // 2
    far = chips // 2
    core = lax.rem(sp, 2)
    chip = sp // 2
    twin = sp + 1 - 2 * core
    after = lax.rem(sp + 1, num_sp)
    before = lax.rem(sp + num_sp - 1, num_sp)
    z_next = (lax.rem(sp + 2, num_sp), lax.rem(sp + num_sp - 2, num_sp))
    t_next = (lax.rem(t + 1, num_tp), lax.rem(t + num_tp - 1, num_tp))
    place = lax.rem(sp, TEAM)
    team = sp // TEAM
    teams = num_sp // TEAM

    def sp_id(index):
        return {"sp": index}

    def tp_id(index):
        return {"tp": index}

    def mate(k):
        return team * TEAM + lax.rem(place + k, TEAM)

    def far_mate(k):
        return lax.rem(sp + TEAM * k, num_sp)

    barrier = pltpu.get_barrier_semaphore()
    partners = [sp_id(after), sp_id(before), sp_id(z_next[0]), sp_id(z_next[1])]
    partners += [sp_id(mate(k)) for k in range(1, TEAM)]
    partners += [sp_id(far_mate(k)) for k in range(1, teams)]
    partners += [tp_id(lax.rem(t + k, num_tp)) for k in range(1, num_tp)]
    partners += [{"grp": pair_grp}]
    for partner in partners:
        pl.semaphore_signal(barrier, inc=1, device_id=partner, device_id_type=pl.DeviceIdType.MESH)

    own_rows = aligned(sp * shard, shard, shard)

    def weight_loads():
        copies = []
        for j in range(tiles):
            for side, source in enumerate((gw_hbm, vw_hbm)):
                copies.append(
                    pltpu.make_async_copy(
                        source.at[:, pl.ds(j * LANES, LANES)],
                        wgv.at[own_rows, pl.ds((2 * j + side) * LANES, LANES)],
                        wload_sem.at[2 * j + side],
                    )
                )
        copies.append(pltpu.make_async_copy(dw_hbm, wd.at[own_rows, :], wload_sem.at[2 * tiles]))
        return copies

    mix_load = pltpu.make_async_copy(mix_hbm, mixb, load_sem.at[0])
    jump_loads = [
        pltpu.make_async_copy(
            jump_hbm.at[:, pl.ds(g * LANES, LANES)], a_s.at[g], load_sem.at[5 + g]
        )
        for g in range(groups)
    ]
    gate_load = pltpu.make_async_copy(gate_hbm, gateb, load_sem.at[1])
    outw_load = pltpu.make_async_copy(outw_hbm, outw, load_sem.at[2])
    resid_load = pltpu.make_async_copy(
        resid_hbm.at[aligned(t * rows, rows, 16), :], resid, load_sem.at[3]
    )
    mix_load.start()
    loads = weight_loads()
    for copy in loads:
        copy.start()
    for copy in jump_loads:
        copy.start()
    gate_load.start()
    outw_load.start()
    resid_load.start()
    for g in range(groups):
        maps[g, :, :LANES] = recur_map[g]
        maps[g, :, LANES:] = input_map[g]

    whole = (wgv, wd)
    lone = ((2 * tiles // 3) * LANES, ((tiles + 1) // 3) * LANES)
    near = 2 * (far - 1)
    per_stage = near + 1

    def part_ref(stage, origin, part, side):
        ref, size = whole[stage], lone[stage]
        at = aligned((2 * origin + core) * shard, shard, shard)
        if part == 0:
            return ref.at[at, aligned(side * size, size, LANES)]
        return ref.at[at, pl.ds(2 * size, ref.shape[1] - 2 * size)]

    def origin_at(way, distance):
        return lax.rem(chip + (chips - distance if way == 0 else distance), chips)

    def what(way, index):
        return index // 2 + 1, (way if index == near else index % 2)

    def remote(ref, send_sem, recv_sem, device_id):
        return pltpu.make_async_remote_copy(
            src_ref=ref,
            dst_ref=ref,
            send_sem=send_sem,
            recv_sem=recv_sem,
            device_id=device_id,
            device_id_type=pl.DeviceIdType.MESH,
        )

    def ring_copy(way, stage, index, received=False):
        distance, part = what(way, index)
        ref = part_ref(stage, origin_at(way, distance - (0 if received else 1)), part, parity)
        slot = stage * per_stage + index
        return remote(
            ref, ring_send.at[way, slot], ring_recv.at[way, slot], sp_id(z_next[way])
        )

    def pair_copy(way, stage, distance, received=False):
        side = 1 - parity if received else parity
        ref = part_ref(stage, origin_at(way, distance), 0, side)
        slot = stage * per_stage + way * far + distance - 1
        return remote(ref, pair_send.at[slot], pair_recv.at[slot], {"grp": pair_grp})

    def twin_copy(ref, stage):
        return remote(ref, twin_send.at[stage], twin_recv.at[stage], sp_id(twin))

    def arrived(way, stage, index):
        distance, part = what(way, index)
        ring_copy(way, stage, index, True).wait_recv()
        if distance < far - 1:
            ring_copy(way, stage, index + 2).start()
        elif distance == far - 1 and part == way:
            ring_copy(way, stage, near).start()
        if part == 0:
            pair_copy(way, stage, distance).start()
        twin_copy(part_ref(stage, origin_at(way, distance), part, parity), stage).start()

    def crossed(way, stage, distance):
        pair_copy(way, stage, distance, True).wait_recv()
        twin_copy(part_ref(stage, origin_at(way, distance), 0, 1 - parity), stage).start()

    def ring_start(stage, part):
        for way in range(2):
            ring_copy(way, stage, part).start()

    def event(stage, index):
        if index < per_stage:
            for way in range(2):
                arrived(way, stage, index)
            if index % 2 == 1 and index > 1:
                for way in range(2):
                    crossed(way, stage, (index - 1) // 2)
        else:
            for way in range(2):
                crossed(way, stage, far - 1)
            crossed(0, stage, far)

    def at_distance(stage, distance):
        first = 2 * (distance - 1)
        return [(stage, k) for k in range(first, min(first + 2, per_stage))]

    lag = far - 3
    events = []
    for distance in range(1, far + 1):
        events += at_distance(0, distance)
        if distance > lag:
            events += at_distance(1, distance - lag)
        if distance == lag:
            down_start = len(events)
    events.append((0, per_stage))
    first_done = len(events)
    for distance in range(far - lag + 1, far + 1):
        events += at_distance(1, distance)
    events.append((1, per_stage))
    progress = [0]

    def pump(count):
        for _ in range(count):
            number = progress[0]
            if number >= len(events):
                return
            if number == down_start:
                ring_start(1, 0)
                ring_start(1, 1)
                twin_copy(wd.at[own_rows, :], 1).start()
            event(*events[number])
            progress[0] = number + 1

    mix_load.wait()
    for g in range(groups):
        jump_loads[g].wait()
    xpad[pl.ds(8, length), :] = mixb[...].astype(jnp.float32)
    taps = mix_kernel[...].astype(jnp.float32)
    coef = -GATE_SCALE * softplus(-decay_param[...])
    chunk = 64

    def gates(i):
        for g in range(groups):
            lanes = slice(g * LANES, (g + 1) * LANES)
            window = xpad[aligned(i * chunk, chunk + 8, 8), lanes]
            total = window[8:] * taps[3:4, lanes]
            for back in range(1, 4):
                total += pltpu.roll(window, back, 0)[8:] * taps[3 - back : 4 - back, lanes]
            conv = total.astype(jnp.bfloat16)
            both = jnp.dot(conv, maps[g], preferred_element_type=jnp.float32)
            at = aligned(i * chunk, chunk, 8)
            log_decay = sigmoid(both[:, :LANES]) * coef[:, lanes] + a_s[g, at, :]
            decay = jnp.exp(log_decay)
            loss = -jnp.tanh(log_decay) * (decay * decay + 1.0)
            drive = jnp.sqrt(loss) * sigmoid(both[:, LANES:]) * conv.astype(jnp.float32)
            a_s[g, at, :] = decay
            b_s[g, at, :] = drive

    pl.loop(1, length // chunk)(gates)
    gate_load.wait()
    chunk2 = 176

    def gate_values(i):
        at = aligned(i * chunk2, chunk2, 16)
        for g in range(groups):
            gel[g, at, :] = gelu(gateb[at, g * LANES : (g + 1) * LANES].astype(jnp.float32))

    pl.semaphore_wait(barrier, len(partners))

    halo_copy = pltpu.make_async_remote_copy(
        src_ref=mix_hbm.at[pl.ds(length - 16, 16), :],
        dst_ref=halo,
        send_sem=halo_sem.at[0],
        recv_sem=halo_sem.at[1],
        device_id=sp_id(after),
        device_id_type=pl.DeviceIdType.MESH,
    )
    halo_copy.start()
    for copy in loads:
        copy.wait()
    ring_start(0, 0)
    pl.loop(0, length // chunk2)(gate_values)
    halo_copy.wait_recv()
    edge = halo[...].astype(jnp.float32)[8:, :]
    xpad[pl.ds(0, 8), :] = jnp.where(sp > 0, edge, 0.0)
    gates(0)

    stretch = length // SEGMENTS

    def scan_step(i, carry):
        result = []
        for g in range(groups):
            product, state = carry[g]
            at = pl.ds(i, SEGMENTS, stride=stretch)
            decay = a_s[g, at, :]
            state = decay * state + b_s[g, at, :]
            product = product * decay
            a_s[g, at, :] = product
            b_s[g, at, :] = state
            result.append((product, state))
        return tuple(result)

    unit = jnp.ones((SEGMENTS, LANES), jnp.float32)
    ends = lax.fori_loop(0, stretch, scan_step, tuple((unit, unit * 0.0) for _ in range(groups)), unroll=4)
    segments = []
    for g in range(groups):
        product, state = ends[g]
        passed, held = unit[:1], unit[:1] * 0.0
        firsts, seconds = [], []
        for s in range(SEGMENTS):
            firsts.append(passed)
            seconds.append(held)
            held = product[s : s + 1] * held + state[s : s + 1]
            passed = passed * product[s : s + 1]
        segments.append((jnp.concatenate(firsts, axis=0), jnp.concatenate(seconds, axis=0)))
        own_ab[0:1, pl.ds(g * LANES, LANES)] = passed
        own_ab[1:2, pl.ds(g * LANES, LANES)] = held

    def team_copy(k):
        return pltpu.make_async_remote_copy(
            src_ref=own_ab,
            dst_ref=team_ab.at[TEAM - 1 - k],
            send_sem=team_send.at[k - 1],
            recv_sem=team_recv.at[k - 1],
            device_id=sp_id(mate(k)),
            device_id_type=pl.DeviceIdType.MESH,
        )

    def far_copy(k):
        return pltpu.make_async_remote_copy(
            src_ref=team_total,
            dst_ref=far_ab.at[k - 1],
            send_sem=far_send.at[k - 1],
            recv_sem=far_recv.at[k - 1],
            device_id=sp_id(far_mate(k)),
            device_id_type=pl.DeviceIdType.MESH,
        )

    for k in range(1, TEAM):
        team_copy(k).start()
    ring_start(0, 1)
    twin_copy(wgv.at[own_rows, :], 0).start()
    pump(1)

    for k in range(1, TEAM):
        team_copy(k).wait_recv()
    own = own_ab[...]
    head_a, head_b = jnp.ones_like(own[0:1]), jnp.zeros_like(own[0:1])
    tail_a, tail_b = own[0:1], own[1:2]
    for k in range(TEAM - 1, 0, -1):
        pair = team_ab[TEAM - 1 - k]
        inside = k <= place
        head_b = jnp.where(inside, pair[0:1] * head_b + pair[1:2], head_b)
        head_a = jnp.where(inside, pair[0:1] * head_a, head_a)
    for k in range(TEAM - 1, 0, -1):
        pair = team_ab[TEAM - 1 - k]
        behind = k > place
        tail_b = jnp.where(behind, pair[0:1] * tail_b + pair[1:2], tail_b)
        tail_a = jnp.where(behind, pair[0:1] * tail_a, tail_a)
    team_total[0:1, :] = head_a * tail_a
    team_total[1:2, :] = tail_a * head_b + tail_b
    for k in range(1, teams):
        far_copy(k).start()

    early = range(progress[0], progress[0] + 3)
    progress[0] += 3

    @pl.when(team > 0)
    def _():
        for number in early[:2]:
            event(*events[number])

    reached[...] = jnp.zeros_like(reached)
    for k in range(teams - 1, 0, -1):

        @pl.when(k <= team)
        def _():
            far_copy(k).wait_recv()
            pair = far_ab[k - 1]
            reached[...] = pair[0:1] * reached[...] + pair[1:2]

    carried = head_a * reached[...] + head_b

    @pl.when(team > 0)
    def _():
        event(*events[early[2]])


    inflow = [
        segments[g][0] * carried[:, g * LANES : (g + 1) * LANES] + segments[g][1]
        for g in range(groups)
    ]

    def finish_step(i):
        for g in range(groups):
            at = pl.ds(i, SEGMENTS, stride=stretch)
            state = a_s[g, at, :] * inflow[g] + b_s[g, at, :]
            b_s[g, at, :] = state * gel[g, at, :]

    pl.loop(0, stretch, unroll=8)(finish_step)
    for g in range(groups):
        branch[:, pl.ds(g * LANES, LANES)] = b_s[g].astype(jnp.bfloat16)
    outw_load.wait()

    def reduce_scatter(partial, send, recv, ssem, rsem, finish, pumps, between):
        copies = {}

        def term(s, q, way):
            shift = num_tp - 1 - s if way == 0 else 1 + s
            return partial(lax.rem(t + shift, num_tp), way * half + q * sub)

        for s in range(num_tp):
            for q in range(2):
                for way in range(2):
                    if s == 0:
                        value = term(s, q, way)
                    else:
                        copies[s - 1, q, way].wait_recv()
                        value = ahead[way, q] + recv[way, s - 1, q].astype(jnp.float32)
                    if s < num_tp - 1:
                        send[way, s, q] = value.astype(jnp.bfloat16)
                        copy = pltpu.make_async_remote_copy(
                            src_ref=send.at[way, s, q],
                            dst_ref=recv.at[way, s, q],
                            send_sem=ssem.at[way, s, q],
                            recv_sem=rsem.at[way, s, q],
                            device_id=tp_id(t_next[way]),
                            device_id_type=pl.DeviceIdType.MESH,
                        )
                        copy.start()
                        copies[s, q, way] = copy
                    else:
                        finish(way * half + q * sub, value)
                if s == 0 and q == 0:
                    between()
                if s < num_tp - 1:
                    for way in range(2):
                        ahead[way, q] = term(s + 1, q, way)
                pump(pumps[2 * s + q])
        return list(copies.values())

    def mix_partial(block, column):
        return jnp.dot(
            branch[aligned(block * rows, rows, 16), :],
            outw[:, pl.ds(column, sub)],
            preferred_element_type=jnp.float32,
        )

    def keep_mixed(column, value):
        mixed[:, pl.ds(column, sub)] = value.astype(jnp.bfloat16)

    def early_events():
        @pl.when(team == 0)
        def _():
            for number in early:
                event(*events[number])

    rs1_copies = reduce_scatter(
        mix_partial,
        rs1_send,
        rs1_recv,
        rs1_ssem,
        rs1_rsem,
        keep_mixed,
        (1, 2, 1, 2, 1, 2, 1, 1),
        early_events,
    )
    resid_load.wait()

    def scaled(value, gain):
        mean = jnp.mean(value * value, axis=-1, keepdims=True)
        return value * lax.rsqrt(mean + EPS) * gain[...]

    def norm_rows(i):
        at = aligned(i * 16, 16, 16)
        stream = resid[at, :].astype(jnp.float32)
        stream += scaled(mixed[at, :].astype(jnp.float32), mix_gain)
        stream = stream.astype(jnp.bfloat16)
        hidden[at, :] = stream
        normed[aligned(t * rows + i * 16, 16, 16), :] = scaled(
            stream.astype(jnp.float32), inner_gain
        ).astype(jnp.bfloat16)

    cut = (rows // 32 + 1) * 16
    parts = ((0, cut), (cut, rows - cut))
    order = tuple(
        tuple((part, side) for part in range(2) for side in (way, 1 - way))
        + tuple((part, way) for part in range(2))
        for way in range(2)
    )

    def gather_ref(way, index, hops):
        part, side = order[way][index]
        block = lax.rem(t + (num_tp - hops if way == 0 else hops), num_tp)
        first, size = parts[part]
        return normed.at[aligned(block * rows + first, size, 16), pl.ds(side * half, half)]

    def gather_copy(way, index):
        ref = gather_ref(way, index, 0 if index < 4 else 1)
        return remote(ref, ag_ssem.at[way, index], ag_rsem.at[way, index], tp_id(t_next[way]))

    def gather_wait(way, index):
        ref = gather_ref(way, index, 1 if index < 4 else 2)
        remote(
            ref, ag_ssem.at[way, index], ag_rsem.at[way, index], tp_id(t_next[way])
        ).wait_recv()

    for part in range(2):
        first, size = parts[part]
        pl.loop(first // 16, (first + size) // 16, unroll=size // 16)(norm_rows)
        for index in range(2 * part, 2 * part + 2):
            for way in range(2):
                gather_copy(way, index).start()
    pump(4)
    for way in range(2):
        gather_wait(way, 0)
        gather_copy(way, 4).start()
    pump(3)
    for way in range(2):
        gather_wait(way, 1)
        gather_wait(way, 2)
        gather_copy(way, 5).start()

    tail_copy = pltpu.make_async_remote_copy(
        src_ref=up.at[pl.ds(length, 16), :],
        dst_ref=up.at[pl.ds(0, 16), :],
        send_sem=tail_sem.at[0],
        recv_sem=tail_sem.at[1],
        device_id=sp_id(after),
        device_id_type=pl.DeviceIdType.MESH,
    )

    def act_ready(block):
        @pl.when(block == 0)
        def _():
            tail_copy.wait_recv()

            @pl.when(sp == 0)
            def _():
                up[pl.ds(0, 16), :] = jnp.zeros((16, 2 * width), jnp.bfloat16)

    def act_tile(block, j):
        columns = aligned(j * LANES, LANES, LANES)
        results = []
        for side, kernel in enumerate((gate_kernel, value_kernel)):
            start = (2 * j + side) * LANES
            value = up[
                aligned(block * rows, rows + 16, 16), aligned(start, LANES, LANES)
            ].astype(jnp.float32)
            tap = kernel[:, columns].astype(jnp.float32)
            total = value[16:] * tap[2:3]
            for back in range(1, 3):
                total += pltpu.roll(value, back, 0)[16:] * tap[2 - back : 3 - back]
            results.append(total)
        act[aligned(block * rows, rows, 16), columns] = (gelu(results[0]) * results[1]).astype(
            jnp.bfloat16
        )

    def act_block(block):
        act_ready(block)
        pl.loop(0, tiles)(lambda j: act_tile(block, j))

    def up_block(block, beside=None):
        if beside is not None:
            act_ready(beside)

        def tile(j):
            columns = aligned(j * 2 * LANES, 2 * LANES, LANES)
            if beside is not None:
                act_tile(beside, j)
            up[aligned(16 + block * rows, rows, 16), columns] = jnp.dot(
                normed[aligned(block * rows, rows, 16), :],
                wgv[:, columns],
                preferred_element_type=jnp.float32,
            ).astype(jnp.bfloat16)

        pl.loop(0, tiles, unroll=tiles)(tile)

        @pl.when(block == num_tp - 1)
        def _():
            tail_copy.start()

    def around(k):
        return lax.rem(t + k, num_tp)

    pump(first_done + 2 - progress[0])
    rival = wgv.at[pl.ds(0, chips * shard), :]
    pltpu.make_async_copy(rival, rival, twin_recv.at[0]).wait()
    up_block(around(0))
    pump(2)
    gather_wait(0, 3)
    up_block(around(num_tp - 1))
    pump(2)
    gather_wait(1, 3)
    up_block(around(1))
    pump(2)
    act_block(around(0))
    pump(1)
    for index in range(4, 6):
        for way in range(2):
            gather_wait(way, index)
    up_block(around(2), around(1))
    pump(1)
    act_block(around(num_tp - 1))
    pump(len(events))
    rival = wd.at[pl.ds(0, chips * shard), :]
    pltpu.make_async_copy(rival, rival, twin_recv.at[1]).wait()

    def down_partial(block, column):
        return lax.dot_general(
            act[aligned(block * rows, rows, 16), :],
            wd[pl.ds(column, sub), :],
            (((1,), (1,)), ((), ())),
            preferred_element_type=jnp.float32,
        )

    rs2_copies = reduce_scatter(
        down_partial,
        rs2_send,
        rs2_recv,
        rs2_ssem,
        rs2_rsem,
        keep_mixed,
        (0,) * 8,
        lambda: act_block(around(2)),
    )

    def last_rows(i):
        at = aligned(i * 16, 16, 16)
        stream = hidden[at, :].astype(jnp.float32)
        stream += scaled(mixed[at, :].astype(jnp.float32), final_gain)
        out_ref[at, :] = stream.astype(jnp.bfloat16)

    pl.loop(0, rows // 16, unroll=rows // 16)(last_rows)

    halo_copy.wait_send()
    tail_copy.wait_send()
    for k in range(1, TEAM):
        team_copy(k).wait_send()
    for k in range(1, teams):
        far_copy(k).wait_send()

        @pl.when(k > team)
        def _():
            far_copy(k).wait_recv()

    for stage in range(2):
        for way in range(2):
            for index in range(per_stage):
                ring_copy(way, stage, index).wait_send()
            for distance in range(1, far + 1 - way):
                pair_copy(way, stage, distance).wait_send()
    gathered = wgv.at[pl.ds(0, chips * shard), :]
    pltpu.make_async_copy(gathered, gathered, twin_send.at[0]).wait()
    gathered = wd.at[pl.ds(0, chips * shard), :]
    pltpu.make_async_copy(gathered, gathered, twin_send.at[1]).wait()
    for copy in rs1_copies + rs2_copies:
        copy.wait_send()
    for index in range(6):
        for way in range(2):
            gather_copy(way, index).wait_send()


def local(
    num_sp,
    num_tp,
    residual,
    mix_input,
    gate_input,
    mix_kernel,
    recur_gate_map,
    input_gate_map,
    decay_param,
    jump_log,
    out_weight,
    mix_gain,
    inner_gain,
    final_gain,
    gate_weight,
    value_weight,
    gate_kernel,
    value_kernel,
    down_weight,
):
    length, channels = mix_input.shape
    model = residual.shape[1]
    shard, width = gate_weight.shape
    rows = length // num_tp
    sub = model // 4
    groups = channels // LANES
    far = num_sp // 4
    steps = 2 * (2 * far - 1)
    hbm = pl.BlockSpec(memory_space=pl.ANY)
    vmem = pl.BlockSpec(memory_space=pltpu.VMEM)
    bf16, f32 = jnp.bfloat16, jnp.float32
    dma = pltpu.SemaphoreType.DMA
    flow = (2, num_tp - 1, 2, rows, sub)
    return pl.pallas_call(
        functools.partial(layer_kernel, num_sp, num_tp),
        out_shape=jax.ShapeDtypeStruct((rows, model), bf16),
        in_specs=[hbm] * 8 + [vmem] * 9,
        out_specs=vmem,
        scratch_shapes=[
            pltpu.VMEM((num_sp * shard, 2 * width), bf16),
            pltpu.VMEM((num_sp * shard, width), bf16),
            pltpu.VMEM((length, channels), bf16),
            pltpu.VMEM((16, channels), bf16),
            pltpu.VMEM((length, channels), bf16),
            pltpu.VMEM((groups, length, LANES), f32),
            pltpu.VMEM((groups, length, LANES), f32),
            pltpu.VMEM((groups, length, LANES), f32),
            pltpu.VMEM((length + 8, channels), f32),
            pltpu.VMEM((groups, LANES, 2 * LANES), bf16),
            pltpu.VMEM((length, channels), bf16),
            pltpu.VMEM((channels, model), bf16),
            pltpu.VMEM((rows, model), bf16),
            pltpu.VMEM((2, channels), f32),
            pltpu.VMEM((TEAM - 1, 2, channels), f32),
            pltpu.VMEM((2, channels), f32),
            pltpu.VMEM((num_sp // TEAM - 1, 2, channels), f32),
            pltpu.VMEM((1, channels), f32),
            pltpu.VMEM(flow, bf16),
            pltpu.VMEM(flow, bf16),
            pltpu.VMEM(flow, bf16),
            pltpu.VMEM(flow, bf16),
            pltpu.VMEM((2, 2, rows, sub), f32),
            pltpu.VMEM((rows, model), bf16),
            pltpu.VMEM((rows, model), bf16),
            pltpu.VMEM((length, model), bf16),
            pltpu.VMEM((16 + length, 2 * width), bf16),
            pltpu.VMEM((length, width), bf16),
            dma((5 + groups,)),
            dma((2 * (width // LANES) + 1,)),
            dma((2,)),
            dma((2,)),
            dma((TEAM - 1,)),
            dma((TEAM - 1,)),
            dma((num_sp // TEAM - 1,)),
            dma((num_sp // TEAM - 1,)),
            dma((2, steps)),
            dma((2, steps)),
            dma((steps,)),
            dma((steps,)),
            dma((2,)),
            dma((2,)),
            dma(flow[:3]),
            dma(flow[:3]),
            dma(flow[:3]),
            dma(flow[:3]),
            dma((2, 6)),
            dma((2, 6)),
        ],
        compiler_params=pltpu.CompilerParams(
            collective_id=0, has_side_effects=True, vmem_limit_bytes=67043328
        ),
    )(
        mix_input,
        gate_input,
        jump_log,
        residual,
        out_weight,
        gate_weight,
        value_weight,
        down_weight.T,
        mix_kernel,
        recur_gate_map,
        input_gate_map,
        decay_param.reshape(1, channels),
        mix_gain.reshape(1, model),
        inner_gain.reshape(1, model),
        final_gain.reshape(1, model),
        gate_kernel,
        value_kernel,
    )


def solution(mesh):
    return jax.shard_map(
        functools.partial(local, mesh.shape["sp"], mesh.shape["tp"]),
        mesh=mesh,
        in_specs=(
            P(("grp", "sp"), None),
            P(("grp", "sp"), "tp"),
            P(("grp", "sp"), "tp"),
            P(None, "tp"),
            P("tp", None, None),
            P("tp", None, None),
            P("tp"),
            P(("grp", "sp"), "tp"),
            P("tp", None),
            P(),
            P(),
            P(),
            P("sp", "tp"),
            P("sp", "tp"),
            P(None, "tp"),
            P(None, "tp"),
            P("tp", "sp"),
        ),
        out_specs=P(("grp", "sp", "tp"), None),
        check_vma=False,
    )
```

```python
import functools

import jax
import jax.numpy as jnp
from jax import lax
from jax.experimental import pallas as pl
from jax.experimental.pallas import tpu as pltpu
from jax.sharding import PartitionSpec as P

EPS = 1e-06
GATE_SCALE = 8.0
LANES = 128
SEGMENTS = 8
TEAM = 8
SQRT_2_PI = 0.7978845608028654


def gelu(v):
    return 0.5 * v * (1.0 + jnp.tanh(SQRT_2_PI * (v + 0.044715 * (v * v * v))))


def sigmoid(v):
    return 1.0 / (1.0 + jnp.exp(-v))


def softplus(v):
    z = jnp.exp(-jnp.abs(v))
    ratio = z / (2.0 + z)
    square = ratio * ratio
    series = jnp.full_like(square, 1.0 / 19.0)
    for power in range(17, 0, -2):
        series = series * square + 1.0 / power
    return jnp.maximum(v, 0.0) + 2.0 * ratio * series


def aligned(start, size, multiple):
    return pl.ds(pl.multiple_of(start, multiple), size)


def layer_kernel(
    num_sp,
    num_tp,
    mix_hbm,
    gate_hbm,
    jump_hbm,
    resid_hbm,
    outw_hbm,
    gw_hbm,
    vw_hbm,
    dw_hbm,
    mix_kernel,
    recur_map,
    input_map,
    decay_param,
    mix_gain,
    inner_gain,
    final_gain,
    gate_kernel,
    value_kernel,
    out_ref,
    wgv,
    wd,
    mixb,
    halo,
    gateb,
    a_s,
    b_s,
    gel,
    xpad,
    maps,
    branch,
    outw,
    resid,
    own_ab,
    team_ab,
    team_total,
    far_ab,
    reached,
    rs1_send,
    rs1_recv,
    rs2_send,
    rs2_recv,
    ahead,
    mixed,
    hidden,
    normed,
    up,
    act,
    load_sem,
    wload_sem,
    halo_sem,
    tail_sem,
    team_send,
    team_recv,
    far_send,
    far_recv,
    ring_send,
    ring_recv,
    pair_send,
    pair_recv,
    twin_send,
    twin_recv,
    rs1_ssem,
    rs1_rsem,
    rs2_ssem,
    rs2_rsem,
    ag_ssem,
    ag_rsem,
):
    sp = lax.axis_index("sp")
    grp = lax.axis_index("grp")
    parity = lax.rem(grp, 2)
    pair_grp = grp + 1 - 2 * parity
    t = lax.axis_index("tp")
    length, channels = mixb.shape
    groups = channels // LANES
    shard = gw_hbm.shape[0]
    width = gw_hbm.shape[1]
    tiles = width // LANES
    model = outw.shape[1]
    rows = length // num_tp
    half = model // 2
    sub = half // 2
    chips = num_sp // 2
    far = chips // 2
    core = lax.rem(sp, 2)
    chip = sp // 2
    twin = sp + 1 - 2 * core
    after = lax.rem(sp + 1, num_sp)
    before = lax.rem(sp + num_sp - 1, num_sp)
    z_next = (lax.rem(sp + 2, num_sp), lax.rem(sp + num_sp - 2, num_sp))
    t_next = (lax.rem(t + 1, num_tp), lax.rem(t + num_tp - 1, num_tp))
    place = lax.rem(sp, TEAM)
    team = sp // TEAM
    teams = num_sp // TEAM

    def sp_id(index):
        return {"sp": index}

    def tp_id(index):
        return {"tp": index}

    def mate(k):
        return team * TEAM + lax.rem(place + k, TEAM)

    def far_mate(k):
        return lax.rem(sp + TEAM * k, num_sp)

    barrier = pltpu.get_barrier_semaphore()
    partners = [sp_id(after), sp_id(before), sp_id(z_next[0]), sp_id(z_next[1])]
    partners += [sp_id(mate(k)) for k in range(1, TEAM)]
    partners += [sp_id(far_mate(k)) for k in range(1, teams)]
    partners += [tp_id(lax.rem(t + k, num_tp)) for k in range(1, num_tp)]
    partners += [{"grp": pair_grp}]
    for partner in partners:
        pl.semaphore_signal(barrier, inc=1, device_id=partner, device_id_type=pl.DeviceIdType.MESH)

    own_rows = aligned(sp * shard, shard, shard)

    def weight_loads():
        copies = []
        for j in range(tiles):
            for side, source in enumerate((gw_hbm, vw_hbm)):
                copies.append(
                    pltpu.make_async_copy(
                        source.at[:, pl.ds(j * LANES, LANES)],
                        wgv.at[own_rows, pl.ds((2 * j + side) * LANES, LANES)],
                        wload_sem.at[2 * j + side],
                    )
                )
        copies.append(pltpu.make_async_copy(dw_hbm, wd.at[own_rows, :], wload_sem.at[2 * tiles]))
        return copies

    mix_load = pltpu.make_async_copy(mix_hbm, mixb, load_sem.at[0])
    jump_loads = [
        pltpu.make_async_copy(
            jump_hbm.at[:, pl.ds(g * LANES, LANES)], a_s.at[g], load_sem.at[5 + g]
        )
        for g in range(groups)
    ]
    gate_load = pltpu.make_async_copy(gate_hbm, gateb, load_sem.at[1])
    outw_load = pltpu.make_async_copy(outw_hbm, outw, load_sem.at[2])
    resid_load = pltpu.make_async_copy(
        resid_hbm.at[aligned(t * rows, rows, 16), :], resid, load_sem.at[3]
    )
    mix_load.start()
    loads = weight_loads()
    for copy in loads:
        copy.start()
    for copy in jump_loads:
        copy.start()
    gate_load.start()
    outw_load.start()
    resid_load.start()
    for g in range(groups):
        maps[g, :, :LANES] = recur_map[g]
        maps[g, :, LANES:] = input_map[g]

    whole = (wgv, wd)
    lone = ((2 * tiles // 3) * LANES, ((tiles + 1) // 3) * LANES)
    near = 2 * (far - 1)
    per_stage = near + 1

    def part_ref(stage, origin, part, side):
        ref, size = whole[stage], lone[stage]
        at = aligned((2 * origin + core) * shard, shard, shard)
        if part == 0:
            return ref.at[at, aligned(side * size, size, LANES)]
        return ref.at[at, pl.ds(2 * size, ref.shape[1] - 2 * size)]

    def origin_at(way, distance):
        return lax.rem(chip + (chips - distance if way == 0 else distance), chips)

    def what(way, index):
        return index // 2 + 1, (way if index == near else index % 2)

    def remote(ref, send_sem, recv_sem, device_id):
        return pltpu.make_async_remote_copy(
            src_ref=ref,
            dst_ref=ref,
            send_sem=send_sem,
            recv_sem=recv_sem,
            device_id=device_id,
            device_id_type=pl.DeviceIdType.MESH,
        )

    def ring_copy(way, stage, index, received=False):
        distance, part = what(way, index)
        ref = part_ref(stage, origin_at(way, distance - (0 if received else 1)), part, parity)
        slot = stage * per_stage + index
        return remote(
            ref, ring_send.at[way, slot], ring_recv.at[way, slot], sp_id(z_next[way])
        )

    def pair_copy(way, stage, distance, received=False):
        side = 1 - parity if received else parity
        ref = part_ref(stage, origin_at(way, distance), 0, side)
        slot = stage * per_stage + way * far + distance - 1
        return remote(ref, pair_send.at[slot], pair_recv.at[slot], {"grp": pair_grp})

    def twin_copy(ref, stage):
        return remote(ref, twin_send.at[stage], twin_recv.at[stage], sp_id(twin))

    def arrived(way, stage, index):
        distance, part = what(way, index)
        ring_copy(way, stage, index, True).wait_recv()
        if distance < far - 1:
            ring_copy(way, stage, index + 2).start()
        elif distance == far - 1 and part == way:
            ring_copy(way, stage, near).start()
        if part == 0:
            pair_copy(way, stage, distance).start()
        twin_copy(part_ref(stage, origin_at(way, distance), part, parity), stage).start()

    def crossed(way, stage, distance):
        pair_copy(way, stage, distance, True).wait_recv()
        twin_copy(part_ref(stage, origin_at(way, distance), 0, 1 - parity), stage).start()

    def ring_start(stage, part):
        for way in range(2):
            ring_copy(way, stage, part).start()

    def event(stage, index):
        if index < per_stage:
            for way in range(2):
                arrived(way, stage, index)
            if index % 2 == 1 and index > 1:
                for way in range(2):
                    crossed(way, stage, (index - 1) // 2)
        else:
            for way in range(2):
                crossed(way, stage, far - 1)
            crossed(0, stage, far)

    def at_distance(stage, distance):
        first = 2 * (distance - 1)
        return [(stage, k) for k in range(first, min(first + 2, per_stage))]

    lag = far - 3
    events = []
    for distance in range(1, far + 1):
        events += at_distance(0, distance)
        if distance > lag:
            events += at_distance(1, distance - lag)
        if distance == lag:
            down_start = len(events)
    events.append((0, per_stage))
    first_done = len(events)
    for distance in range(far - lag + 1, far + 1):
        events += at_distance(1, distance)
    events.append((1, per_stage))
    progress = [0]

    def pump(count):
        for _ in range(count):
            number = progress[0]
            if number >= len(events):
                return
            if number == down_start:
                ring_start(1, 0)
                ring_start(1, 1)
                twin_copy(wd.at[own_rows, :], 1).start()
            event(*events[number])
            progress[0] = number + 1

    mix_load.wait()
    for g in range(groups):
        jump_loads[g].wait()
    xpad[pl.ds(8, length), :] = mixb[...].astype(jnp.float32)
    taps = mix_kernel[...].astype(jnp.float32)
    coef = -GATE_SCALE * softplus(-decay_param[...])
    chunk = 64

    def gates(i):
        for g in range(groups):
            lanes = slice(g * LANES, (g + 1) * LANES)
            window = xpad[aligned(i * chunk, chunk + 8, 8), lanes]
            total = window[8:] * taps[3:4, lanes]
            for back in range(1, 4):
                total += pltpu.roll(window, back, 0)[8:] * taps[3 - back : 4 - back, lanes]
            conv = total.astype(jnp.bfloat16)
            both = jnp.dot(conv, maps[g], preferred_element_type=jnp.float32)
            at = aligned(i * chunk, chunk, 8)
            log_decay = sigmoid(both[:, :LANES]) * coef[:, lanes] + a_s[g, at, :]
            decay = jnp.exp(log_decay)
            loss = -jnp.tanh(log_decay) * (decay * decay + 1.0)
            drive = jnp.sqrt(loss) * sigmoid(both[:, LANES:]) * conv.astype(jnp.float32)
            a_s[g, at, :] = decay
            b_s[g, at, :] = drive

    pl.loop(1, length // chunk)(gates)
    gate_load.wait()
    chunk2 = 176

    def gate_values(i):
        at = aligned(i * chunk2, chunk2, 16)
        for g in range(groups):
            gel[g, at, :] = gelu(gateb[at, g * LANES : (g + 1) * LANES].astype(jnp.float32))

    pl.semaphore_wait(barrier, len(partners))

    halo_copy = pltpu.make_async_remote_copy(
        src_ref=mix_hbm.at[pl.ds(length - 16, 16), :],
        dst_ref=halo,
        send_sem=halo_sem.at[0],
        recv_sem=halo_sem.at[1],
        device_id=sp_id(after),
        device_id_type=pl.DeviceIdType.MESH,
    )
    halo_copy.start()
    for copy in loads:
        copy.wait()
    ring_start(0, 0)
    pl.loop(0, length // chunk2)(gate_values)
    halo_copy.wait_recv()
    edge = halo[...].astype(jnp.float32)[8:, :]
    xpad[pl.ds(0, 8), :] = jnp.where(sp > 0, edge, 0.0)
    gates(0)

    stretch = length // SEGMENTS

    def scan_step(i, carry):
        result = []
        for g in range(groups):
            product, state = carry[g]
            at = pl.ds(i, SEGMENTS, stride=stretch)
            decay = a_s[g, at, :]
            state = decay * state + b_s[g, at, :]
            product = product * decay
            a_s[g, at, :] = product
            b_s[g, at, :] = state
            result.append((product, state))
        return tuple(result)

    unit = jnp.ones((SEGMENTS, LANES), jnp.float32)
    ends = lax.fori_loop(0, stretch, scan_step, tuple((unit, unit * 0.0) for _ in range(groups)), unroll=4)
    segments = []
    for g in range(groups):
        product, state = ends[g]
        passed, held = unit[:1], unit[:1] * 0.0
        firsts, seconds = [], []
        for s in range(SEGMENTS):
            firsts.append(passed)
            seconds.append(held)
            held = product[s : s + 1] * held + state[s : s + 1]
            passed = passed * product[s : s + 1]
        segments.append((jnp.concatenate(firsts, axis=0), jnp.concatenate(seconds, axis=0)))
        own_ab[0:1, pl.ds(g * LANES, LANES)] = passed
        own_ab[1:2, pl.ds(g * LANES, LANES)] = held

    def team_copy(k):
        return pltpu.make_async_remote_copy(
            src_ref=own_ab,
            dst_ref=team_ab.at[TEAM - 1 - k],
            send_sem=team_send.at[k - 1],
            recv_sem=team_recv.at[k - 1],
            device_id=sp_id(mate(k)),
            device_id_type=pl.DeviceIdType.MESH,
        )

    def far_copy(k):
        return pltpu.make_async_remote_copy(
            src_ref=team_total,
            dst_ref=far_ab.at[k - 1],
            send_sem=far_send.at[k - 1],
            recv_sem=far_recv.at[k - 1],
            device_id=sp_id(far_mate(k)),
            device_id_type=pl.DeviceIdType.MESH,
        )

    for k in range(1, TEAM):
        team_copy(k).start()
    ring_start(0, 1)
    twin_copy(wgv.at[own_rows, :], 0).start()
    pump(1)

    for k in range(1, TEAM):
        team_copy(k).wait_recv()
    own = own_ab[...]
    head_a, head_b = jnp.ones_like(own[0:1]), jnp.zeros_like(own[0:1])
    tail_a, tail_b = own[0:1], own[1:2]
    for k in range(TEAM - 1, 0, -1):
        pair = team_ab[TEAM - 1 - k]
        inside = k <= place
        head_b = jnp.where(inside, pair[0:1] * head_b + pair[1:2], head_b)
        head_a = jnp.where(inside, pair[0:1] * head_a, head_a)
    for k in range(TEAM - 1, 0, -1):
        pair = team_ab[TEAM - 1 - k]
        behind = k > place
        tail_b = jnp.where(behind, pair[0:1] * tail_b + pair[1:2], tail_b)
        tail_a = jnp.where(behind, pair[0:1] * tail_a, tail_a)
    team_total[0:1, :] = head_a * tail_a
    team_total[1:2, :] = tail_a * head_b + tail_b
    for k in range(1, teams):
        far_copy(k).start()

    early = range(progress[0], progress[0] + 3)
    progress[0] += 3

    @pl.when(team > 0)
    def _():
        for number in early[:2]:
            event(*events[number])

    reached[...] = jnp.zeros_like(reached)
    for k in range(teams - 1, 0, -1):

        @pl.when(k <= team)
        def _():
            far_copy(k).wait_recv()
            pair = far_ab[k - 1]
            reached[...] = pair[0:1] * reached[...] + pair[1:2]

    carried = head_a * reached[...] + head_b

    @pl.when(team > 0)
    def _():
        event(*events[early[2]])


    inflow = [
        segments[g][0] * carried[:, g * LANES : (g + 1) * LANES] + segments[g][1]
        for g in range(groups)
    ]

    def finish_step(i):
        for g in range(groups):
            at = pl.ds(i, SEGMENTS, stride=stretch)
            state = a_s[g, at, :] * inflow[g] + b_s[g, at, :]
            b_s[g, at, :] = state * gel[g, at, :]

    pl.loop(0, stretch, unroll=8)(finish_step)
    for g in range(groups):
        branch[:, pl.ds(g * LANES, LANES)] = b_s[g].astype(jnp.bfloat16)
    outw_load.wait()

    def reduce_scatter(partial, send, recv, ssem, rsem, finish, pumps, between):
        copies = {}

        def term(s, q, way):
            shift = num_tp - 1 - s if way == 0 else 1 + s
            return partial(lax.rem(t + shift, num_tp), way * half + q * sub)

        for s in range(num_tp):
            for q in range(2):
                for way in range(2):
                    if s == 0:
                        value = term(s, q, way)
                    else:
                        copies[s - 1, q, way].wait_recv()
                        value = ahead[way, q] + recv[way, s - 1, q].astype(jnp.float32)
                    if s < num_tp - 1:
                        send[way, s, q] = value.astype(jnp.bfloat16)
                        copy = pltpu.make_async_remote_copy(
                            src_ref=send.at[way, s, q],
                            dst_ref=recv.at[way, s, q],
                            send_sem=ssem.at[way, s, q],
                            recv_sem=rsem.at[way, s, q],
                            device_id=tp_id(t_next[way]),
                            device_id_type=pl.DeviceIdType.MESH,
                        )
                        copy.start()
                        copies[s, q, way] = copy
                    else:
                        finish(way * half + q * sub, value)
                if s == 0 and q == 0:
                    between()
                if s < num_tp - 1:
                    for way in range(2):
                        ahead[way, q] = term(s + 1, q, way)
                pump(pumps[2 * s + q])
        return list(copies.values())

    def mix_partial(block, column):
        return jnp.dot(
            branch[aligned(block * rows, rows, 16), :],
            outw[:, pl.ds(column, sub)],
            preferred_element_type=jnp.float32,
        )

    def keep_mixed(column, value):
        mixed[:, pl.ds(column, sub)] = value.astype(jnp.bfloat16)

    def early_events():
        @pl.when(team == 0)
        def _():
            for number in early:
                event(*events[number])

    rs1_copies = reduce_scatter(
        mix_partial,
        rs1_send,
        rs1_recv,
        rs1_ssem,
        rs1_rsem,
        keep_mixed,
        (1, 2, 1, 2, 1, 2, 1, 1),
        early_events,
    )
    resid_load.wait()

    def scaled(value, gain):
        mean = jnp.mean(value * value, axis=-1, keepdims=True)
        return value * lax.rsqrt(mean + EPS) * gain[...]

    def norm_rows(i):
        at = aligned(i * 16, 16, 16)
        stream = resid[at, :].astype(jnp.float32)
        stream += scaled(mixed[at, :].astype(jnp.float32), mix_gain)
        stream = stream.astype(jnp.bfloat16)
        hidden[at, :] = stream
        normed[aligned(t * rows + i * 16, 16, 16), :] = scaled(
            stream.astype(jnp.float32), inner_gain
        ).astype(jnp.bfloat16)

    cut = (rows // 32 + 1) * 16
    parts = ((0, cut), (cut, rows - cut))
    order = tuple(
        tuple((part, side) for part in range(2) for side in (way, 1 - way))
        + tuple((part, way) for part in range(2))
        for way in range(2)
    )

    def gather_ref(way, index, hops):
        part, side = order[way][index]
        block = lax.rem(t + (num_tp - hops if way == 0 else hops), num_tp)
        first, size = parts[part]
        return normed.at[aligned(block * rows + first, size, 16), pl.ds(side * half, half)]

    def gather_copy(way, index):
        ref = gather_ref(way, index, 0 if index < 4 else 1)
        return remote(ref, ag_ssem.at[way, index], ag_rsem.at[way, index], tp_id(t_next[way]))

    def gather_wait(way, index):
        ref = gather_ref(way, index, 1 if index < 4 else 2)
        remote(
            ref, ag_ssem.at[way, index], ag_rsem.at[way, index], tp_id(t_next[way])
        ).wait_recv()

    for part in range(2):
        first, size = parts[part]
        pl.loop(first // 16, (first + size) // 16, unroll=size // 16)(norm_rows)
        for index in range(2 * part, 2 * part + 2):
            for way in range(2):
                gather_copy(way, index).start()
    pump(4)
    for way in range(2):
        gather_wait(way, 0)
        gather_copy(way, 4).start()

    tail_copy = pltpu.make_async_remote_copy(
        src_ref=up.at[pl.ds(length, 16), :],
        dst_ref=up.at[pl.ds(0, 16), :],
        send_sem=tail_sem.at[0],
        recv_sem=tail_sem.at[1],
        device_id=sp_id(after),
        device_id_type=pl.DeviceIdType.MESH,
    )

    def act_ready(block):
        @pl.when(block == 0)
        def _():
            tail_copy.wait_recv()

            @pl.when(sp == 0)
            def _():
                up[pl.ds(0, 16), :] = jnp.zeros((16, 2 * width), jnp.bfloat16)

    def act_tile(block, j):
        columns = aligned(j * LANES, LANES, LANES)
        results = []
        for side, kernel in enumerate((gate_kernel, value_kernel)):
            start = (2 * j + side) * LANES
            value = up[
                aligned(block * rows, rows + 16, 16), aligned(start, LANES, LANES)
            ].astype(jnp.float32)
            tap = kernel[:, columns].astype(jnp.float32)
            total = value[16:] * tap[2:3]
            for back in range(1, 3):
                total += pltpu.roll(value, back, 0)[16:] * tap[2 - back : 3 - back]
            results.append(total)
        act[aligned(block * rows, rows, 16), columns] = (gelu(results[0]) * results[1]).astype(
            jnp.bfloat16
        )

    def act_block(block):
        act_ready(block)
        pl.loop(0, tiles)(lambda j: act_tile(block, j))

    def up_block(block, beside=None):
        if beside is not None:
            act_ready(beside)

        def tile(j):
            columns = aligned(j * 2 * LANES, 2 * LANES, LANES)
            if beside is not None:
                act_tile(beside, j)
            up[aligned(16 + block * rows, rows, 16), columns] = jnp.dot(
                normed[aligned(block * rows, rows, 16), :],
                wgv[:, columns],
                preferred_element_type=jnp.float32,
            ).astype(jnp.bfloat16)

        pl.loop(0, tiles, unroll=tiles)(tile)

        @pl.when(block == num_tp - 1)
        def _():
            tail_copy.start()

    def around(k):
        return lax.rem(t + k, num_tp)

    pump(first_done + 2 - progress[0])
    rival = wgv.at[pl.ds(0, chips * shard), :]
    pltpu.make_async_copy(rival, rival, twin_recv.at[0]).wait()
    up_block(around(0))
    for way in range(2):
        gather_wait(way, 1)
        gather_wait(way, 2)
        gather_copy(way, 5).start()
    pump(2)
    gather_wait(0, 3)
    up_block(around(num_tp - 1))
    pump(2)
    gather_wait(1, 3)
    up_block(around(1))
    pump(2)
    act_block(around(0))
    pump(1)
    for index in range(4, 6):
        for way in range(2):
            gather_wait(way, index)
    up_block(around(2), around(1))
    pump(1)
    act_block(around(num_tp - 1))
    pump(len(events))
    rival = wd.at[pl.ds(0, chips * shard), :]
    pltpu.make_async_copy(rival, rival, twin_recv.at[1]).wait()

    def down_partial(block, column):
        return lax.dot_general(
            act[aligned(block * rows, rows, 16), :],
            wd[pl.ds(column, sub), :],
            (((1,), (1,)), ((), ())),
            preferred_element_type=jnp.float32,
        )

    rs2_copies = reduce_scatter(
        down_partial,
        rs2_send,
        rs2_recv,
        rs2_ssem,
        rs2_rsem,
        keep_mixed,
        (0,) * 8,
        lambda: act_block(around(2)),
    )

    def last_rows(i):
        at = aligned(i * 16, 16, 16)
        stream = hidden[at, :].astype(jnp.float32)
        stream += scaled(mixed[at, :].astype(jnp.float32), final_gain)
        out_ref[at, :] = stream.astype(jnp.bfloat16)

    pl.loop(0, rows // 16, unroll=rows // 16)(last_rows)

    halo_copy.wait_send()
    tail_copy.wait_send()
    for k in range(1, TEAM):
        team_copy(k).wait_send()
    for k in range(1, teams):
        far_copy(k).wait_send()

        @pl.when(k > team)
        def _():
            far_copy(k).wait_recv()

    for stage in range(2):
        for way in range(2):
            for index in range(per_stage):
                ring_copy(way, stage, index).wait_send()
            for distance in range(1, far + 1 - way):
                pair_copy(way, stage, distance).wait_send()
    gathered = wgv.at[pl.ds(0, chips * shard), :]
    pltpu.make_async_copy(gathered, gathered, twin_send.at[0]).wait()
    gathered = wd.at[pl.ds(0, chips * shard), :]
    pltpu.make_async_copy(gathered, gathered, twin_send.at[1]).wait()
    for copy in rs1_copies + rs2_copies:
        copy.wait_send()
    for index in range(6):
        for way in range(2):
            gather_copy(way, index).wait_send()


def local(
    num_sp,
    num_tp,
    residual,
    mix_input,
    gate_input,
    mix_kernel,
    recur_gate_map,
    input_gate_map,
    decay_param,
    jump_log,
    out_weight,
    mix_gain,
    inner_gain,
    final_gain,
    gate_weight,
    value_weight,
    gate_kernel,
    value_kernel,
    down_weight,
):
    length, channels = mix_input.shape
    model = residual.shape[1]
    shard, width = gate_weight.shape
    rows = length // num_tp
    sub = model // 4
    groups = channels // LANES
    far = num_sp // 4
    steps = 2 * (2 * far - 1)
    hbm = pl.BlockSpec(memory_space=pl.ANY)
    vmem = pl.BlockSpec(memory_space=pltpu.VMEM)
    bf16, f32 = jnp.bfloat16, jnp.float32
    dma = pltpu.SemaphoreType.DMA
    flow = (2, num_tp - 1, 2, rows, sub)
    return pl.pallas_call(
        functools.partial(layer_kernel, num_sp, num_tp),
        out_shape=jax.ShapeDtypeStruct((rows, model), bf16),
        in_specs=[hbm] * 8 + [vmem] * 9,
        out_specs=vmem,
        scratch_shapes=[
            pltpu.VMEM((num_sp * shard, 2 * width), bf16),
            pltpu.VMEM((num_sp * shard, width), bf16),
            pltpu.VMEM((length, channels), bf16),
            pltpu.VMEM((16, channels), bf16),
            pltpu.VMEM((length, channels), bf16),
            pltpu.VMEM((groups, length, LANES), f32),
            pltpu.VMEM((groups, length, LANES), f32),
            pltpu.VMEM((groups, length, LANES), f32),
            pltpu.VMEM((length + 8, channels), f32),
            pltpu.VMEM((groups, LANES, 2 * LANES), bf16),
            pltpu.VMEM((length, channels), bf16),
            pltpu.VMEM((channels, model), bf16),
            pltpu.VMEM((rows, model), bf16),
            pltpu.VMEM((2, channels), f32),
            pltpu.VMEM((TEAM - 1, 2, channels), f32),
            pltpu.VMEM((2, channels), f32),
            pltpu.VMEM((num_sp // TEAM - 1, 2, channels), f32),
            pltpu.VMEM((1, channels), f32),
            pltpu.VMEM(flow, bf16),
            pltpu.VMEM(flow, bf16),
            pltpu.VMEM(flow, bf16),
            pltpu.VMEM(flow, bf16),
            pltpu.VMEM((2, 2, rows, sub), f32),
            pltpu.VMEM((rows, model), bf16),
            pltpu.VMEM((rows, model), bf16),
            pltpu.VMEM((length, model), bf16),
            pltpu.VMEM((16 + length, 2 * width), bf16),
            pltpu.VMEM((length, width), bf16),
            dma((5 + groups,)),
            dma((2 * (width // LANES) + 1,)),
            dma((2,)),
            dma((2,)),
            dma((TEAM - 1,)),
            dma((TEAM - 1,)),
            dma((num_sp // TEAM - 1,)),
            dma((num_sp // TEAM - 1,)),
            dma((2, steps)),
            dma((2, steps)),
            dma((steps,)),
            dma((steps,)),
            dma((2,)),
            dma((2,)),
            dma(flow[:3]),
            dma(flow[:3]),
            dma(flow[:3]),
            dma(flow[:3]),
            dma((2, 6)),
            dma((2, 6)),
        ],
        compiler_params=pltpu.CompilerParams(
            collective_id=0, has_side_effects=True, vmem_limit_bytes=67043328
        ),
    )(
        mix_input,
        gate_input,
        jump_log,
        residual,
        out_weight,
        gate_weight,
        value_weight,
        down_weight.T,
        mix_kernel,
        recur_gate_map,
        input_gate_map,
        decay_param.reshape(1, channels),
        mix_gain.reshape(1, model),
        inner_gain.reshape(1, model),
        final_gain.reshape(1, model),
        gate_kernel,
        value_kernel,
    )


def solution(mesh):
    return jax.shard_map(
        functools.partial(local, mesh.shape["sp"], mesh.shape["tp"]),
        mesh=mesh,
        in_specs=(
            P(("grp", "sp"), None),
            P(("grp", "sp"), "tp"),
            P(("grp", "sp"), "tp"),
            P(None, "tp"),
            P("tp", None, None),
            P("tp", None, None),
            P("tp"),
            P(("grp", "sp"), "tp"),
            P("tp", None),
            P(),
            P(),
            P(),
            P("sp", "tp"),
            P("sp", "tp"),
            P(None, "tp"),
            P(None, "tp"),
            P("tp", "sp"),
        ),
        out_specs=P(("grp", "sp", "tp"), None),
        check_vma=False,
    )
```
